32 devices in a mesh: ep: 4 (over y, x), tp: 8 (over z, core).
Axes of the slice: x: 2, y: 2, z: 4, core: 2. Of those that a mesh axis runs over, the one named last changes fastest.
Arguments:
- pool_input: bfloat16 [4096, 1024], P('ep', 'tp'), may hold values from -6 to 6
- pool_gain: float32 [1024], P('tp'), may hold values from 0.1 to 1.9
- mix_weight: bfloat16 [1024, 2048], P('tp'), may hold values from -0.1875 to 0.1875
- moe_input: bfloat16 [8192, 2048], P(('ep', 'tp')), may hold values from -6 to 6
- moe_gain: float32 [2048], replicated, may hold values from 0.1 to 1.9
- expert_ids: int32 [8192, 2], P(('ep', 'tp')), may hold values from 0 to 15, as said below
- route_weight: float32 [8192, 2], P(('ep', 'tp')), may hold values from 0.2 to 1
- gate_weight: bfloat16 [16, 2048, 1024], P('ep', None, 'tp'), may hold values from -0.125 to 0.125
- up_weight: bfloat16 [16, 2048, 1024], P('ep', None, 'tp'), may hold values from -0.125 to 0.125
- down_weight: bfloat16 [16, 2048, 1024], P('ep', None, 'tp'), may hold values from -0.1875 to 0.1875
Outputs:
- mixed_out: bfloat16 [4096, 2048], P(('ep', 'tp'))
- moe_out: bfloat16 [8192, 2048], P(('ep', 'tp'))
The draws below stay inside these ranges and needn't reach their ends.
Inputs may be any that keep to these rules, and one draw needn't show every extreme that they name: `expert_ids`: each row names 2 different experts of one group of 4 consecutive experts. In each aligned block of 256 rows (the rows of one device) no expert is named by more than 48 rows, and some expert is named by exactly 48 rows.
All inputs are finite; a program needn't handle non-finite values.
Results may differ from the reference program's by a relative error of at most 0.012.
Values may be sent and summed in bfloat16 or wider, within the bound.
A program may use at most 128 MiB of HBM per device.

```python
import math
import jax
import jax.numpy as jnp
from jax import lax

D = 2048
PW = 1024
GROUP_CH = 256
FF = 1024
EXPERTS = 16
GROUP_EXP = 4
TOP = 2
ROWS_B = 256
CAP = 48
TOK_A = 4096
TOK_B = 8192


def block_routes(block_key):
    subkeys = jax.random.split(block_key, 5)
    remaining = ROWS_B - 2 * CAP
    share_base = remaining // 3
    spread = share_base // 4
    first_shift = jax.random.randint(subkeys[0], (), -spread, spread + 1)
    second_shift = jax.random.randint(subkeys[1], (), -spread, spread + 1)
    others = jnp.stack([share_base + first_shift, share_base + second_shift, remaining - 2 * share_base - first_shift - second_shift]).astype(jnp.int32)
    largest = jax.random.randint(subkeys[2], (), 0, 4)
    group_range = jnp.arange(4, dtype=jnp.int32)
    other_index = jnp.clip(group_range - (group_range > largest).astype(jnp.int32), 0, 2)
    quotas = jnp.where(group_range == largest, 2 * CAP, others[other_index]).astype(jnp.int32)
    group_ends = jnp.cumsum(quotas)
    position = jnp.arange(ROWS_B, dtype=jnp.int32)
    member = jnp.sum((position[:, None] >= group_ends[None, :]).astype(jnp.int32), axis=1)
    within = position - (group_ends - quotas)[member]
    leading = within % 4
    trailing = (within + 1 + within // 4 % 3) % 4
    relabel = jax.random.permutation(subkeys[3], 4).astype(jnp.int32)
    routes = jnp.stack([member * GROUP_EXP + relabel[leading], member * GROUP_EXP + relabel[trailing]], axis=1)
    return routes[jax.random.permutation(subkeys[4], ROWS_B)].astype(jnp.int32)


def draw_expert_ids(key, part):
    block_keys = jax.random.split(jax.random.fold_in(key, 7), TOK_B // ROWS_B)
    return jax.vmap(block_routes)(block_keys).reshape(TOK_B, 2)


def level_of(stream_key, shape, cuts, least, top_value):
    def one(dim, shards_of):
        heights = jax.random.uniform(jax.random.fold_in(jax.random.fold_in(stream_key, 6), dim), (shards_of,), jnp.float32, least / len(cuts), top_value / len(cuts))
        return jnp.repeat(jnp.exp(heights), shape[dim] // shards_of).reshape((-1,) + (1,) * (len(shape) - dim - 1))

    loudness = one(*cuts[0])
    for cut in cuts[1:]:
        loudness = loudness * one(*cut)
    return loudness


def normal_values(stream_key, dims, deviation, limit, cuts=(), kind=jnp.bfloat16):
    result = deviation * jax.random.normal(stream_key, dims, jnp.float32)
    if cuts:
        result = result * level_of(stream_key, dims, cuts, -0.22, 0.18)
    return jnp.clip(result, -limit, limit).astype(kind)


def setup_inputs(seed: int = 0) -> dict:
    key_of = jax.random.split(jax.random.key(seed), 11)
    pool_input = normal_values(key_of[0], (TOK_A, PW), 1.0, 6.0, ((0, 4), (1, 8)))
    pool_gain = jnp.clip(1.0 + 0.18 * jax.random.normal(key_of[1], (PW,), jnp.float32), 0.1, 1.9)
    mix_weight = normal_values(key_of[2], (PW, D), PW ** -0.5, 0.1875, ((0, 8),))
    moe_input = normal_values(key_of[3], (TOK_B, D), 1.0, 6.0, ((0, 32),))
    moe_gain = jnp.clip(1.0 + 0.18 * jax.random.normal(key_of[4], (D,), jnp.float32), 0.1, 1.9)
    expert_ids = draw_expert_ids(jax.random.fold_in(key_of[10], 71), 0)
    route_weight = jnp.clip(jnp.exp(math.log(1.0) - 1.609438 * jax.random.uniform(key_of[6], (TOK_B, TOP), jnp.float32) ** level_of(key_of[6], (TOK_B, TOP), ((0, 32),), -0.2, 0.2)), 0.2, 1.0)
    gate_weight = normal_values(key_of[7], (EXPERTS, D, FF), D ** -0.5, 0.125, ((0, 4), (2, 8)))
    up_weight = normal_values(key_of[8], (EXPERTS, D, FF), D ** -0.5, 0.125, ((0, 4), (2, 8)))
    down_weight = normal_values(key_of[9], (EXPERTS, D, FF), FF ** -0.5, 0.1875, ((0, 4), (2, 8)))
    return dict(pool_input=pool_input, pool_gain=pool_gain, mix_weight=mix_weight, moe_input=moe_input, moe_gain=moe_gain, expert_ids=expert_ids, route_weight=route_weight, gate_weight=gate_weight, up_weight=up_weight, down_weight=down_weight)


eps_norm = 1e-06

def reference(pool_input, pool_gain, mix_weight, moe_input, moe_gain, expert_ids, route_weight, gate_weight, up_weight, down_weight):
    values = pool_input.astype(jnp.float32)
    length = values.shape[0]
    running = jnp.concatenate([jnp.zeros((1, PW), jnp.float32), jnp.cumsum(values, axis=0)], axis=0)
    position = jnp.arange(length, dtype=jnp.int32)
    pieces = []
    for index_group in range(4):
        window = 2 ** (index_group + 1)
        begins = jnp.maximum(position + 1 - window, 0)
        counted = (position + 1 - begins).astype(jnp.float32)
        column = running[:, index_group * GROUP_CH:(index_group + 1) * GROUP_CH]
        pieces.append((column[1:] - column[begins]) / counted[:, None])
    pooled = ((jnp.concatenate(pieces, axis=1) - values) * pool_gain).astype(jnp.bfloat16)
    mixed_out = jnp.dot(pooled, mix_weight, preferred_element_type=jnp.float32).astype(jnp.bfloat16)
    inputs = moe_input.astype(jnp.float32)
    scale_rows = lax.rsqrt(lax.optimization_barrier(jnp.mean(inputs * inputs, axis=-1, keepdims=True)) + eps_norm)
    normed = (inputs * scale_rows * moe_gain).astype(jnp.bfloat16)
    blocks = TOK_B // ROWS_B
    chosen = expert_ids.reshape(blocks, ROWS_B * TOP)
    marked = (chosen[:, :, None] == jnp.arange(EXPERTS, dtype=jnp.int32)[None, None, :]).astype(jnp.int32)
    ranked = lax.optimization_barrier(jnp.sum((jnp.cumsum(marked, axis=1) - marked) * marked, axis=2)).astype(jnp.int32)
    owner_row = (jnp.arange(ROWS_B * TOP, dtype=jnp.int32)[None, :] // TOP + jnp.arange(blocks, dtype=jnp.int32)[:, None] * ROWS_B).astype(jnp.int32)
    block_ids = jnp.broadcast_to(jnp.arange(blocks, dtype=jnp.int32)[:, None], chosen.shape)
    source = jnp.full((EXPERTS, blocks, CAP), TOK_B, jnp.int32).at[chosen, block_ids, ranked].set(owner_row)
    padded = jnp.concatenate([normed, jnp.zeros((1, D), jnp.bfloat16)], axis=0)

    def expert_pass(operands):
        indices, gate_mat, up_mat, down_mat = operands
        gathered = padded[indices.reshape(-1)]
        gate_part = jnp.dot(gathered, gate_mat, preferred_element_type=jnp.float32)
        upward = jnp.dot(gathered, up_mat, preferred_element_type=jnp.float32)
        hidden = (jax.nn.silu(gate_part) * upward).astype(jnp.bfloat16)
        return jnp.dot(hidden, jnp.transpose(down_mat), preferred_element_type=jnp.float32).astype(jnp.bfloat16)
    results = lax.map(expert_pass, (source, gate_weight, up_weight, down_weight))
    flat_index = (chosen * (blocks * CAP) + block_ids * CAP + ranked).astype(jnp.int32)
    picked = results.reshape(EXPERTS * blocks * CAP, D)[flat_index.reshape(-1)].astype(jnp.float32)
    picked = picked.reshape(TOK_B, TOP, D)
    moe_out = lax.optimization_barrier(jnp.sum(picked * route_weight[:, :, None], axis=1)).astype(jnp.bfloat16)
    return (mixed_out, moe_out)
```

```python
import functools

import jax
import jax.numpy as jnp
from jax import lax
from jax.experimental import pallas as pl
from jax.experimental.pallas import tpu as pltpu
from jax.sharding import PartitionSpec as P

GROUP_CH = 256
EXPERTS = 16
GROUP_EXP = 4
TOP = 2
CAP = 48
CHUNKS = 2


eps_norm = 1e-06


def from_behind(shard, axis, by):
    peers = lax.axis_size(axis)
    pairs = [(i, i + by) for i in range(peers) if 0 <= i + by < peers]
    return lax.ppermute(shard, axis, pairs)


def window_sums(extended, row_count):
    level_sum = extended
    stride = 1
    outputs = []
    for doubling in range(4):
        level_sum = level_sum[stride:] + level_sum[:-stride]
        stride = stride * 2
        outputs.append(level_sum[level_sum.shape[0] - row_count :])
    return outputs


def pool_mixer(pool_input, pool_gain):
    row_count, channels = pool_input.shape
    carried = from_behind(pool_input[row_count - 15 :], "ep", 1)
    extended = jnp.concatenate([carried, pool_input], axis=0).astype(jnp.float32)
    window_list = window_sums(extended, row_count)
    channel_ids = lax.axis_index("tp") * channels + lax.iota(jnp.int32, channels)
    group_ids = channel_ids // GROUP_CH
    position = lax.axis_index("ep") * row_count + lax.iota(jnp.int32, row_count)
    summed = jnp.zeros((row_count, channels), jnp.float32)
    widths = jnp.zeros((channels,), jnp.int32)
    for index_group in range(4):
        inside = group_ids == index_group
        summed = jnp.where(inside[None, :], window_list[index_group], summed)
        widths = jnp.where(inside, 2 ** (index_group + 1), widths)
    counted = jnp.minimum(position[:, None] + 1, widths[None, :]).astype(jnp.float32)
    values = extended[15:]
    return ((summed / counted - values) * pool_gain).astype(jnp.bfloat16)


def dispatch_plan(expert_ids, route_weight, ep_size):
    local_experts = EXPERTS // ep_size
    share = TOP if local_experts % GROUP_EXP == 0 else 1
    capacity = local_experts * CAP // share
    owners = expert_ids // local_experts
    ep_index = lax.iota(jnp.int32, ep_size)
    member = jnp.any(owners[:, :, None] == ep_index[None, None, :], axis=1)
    counts = member.astype(jnp.int32)
    rank = jnp.cumsum(counts, axis=0) - counts
    slot = jnp.where(member, rank, -1).T
    placing = slot[:, None, :] == lax.iota(jnp.int32, capacity)[None, :, None]
    dense_weight = jnp.sum(
        jnp.where(
            expert_ids[:, :, None] == lax.iota(jnp.int32, EXPERTS)[None, None, :],
            route_weight[:, :, None],
            0.0,
        ),
        axis=1,
    )
    dense_weight = dense_weight.reshape(-1, ep_size, local_experts)
    slot_weight = jnp.einsum(
        "ecn,nej->ecj",
        placing.astype(jnp.float32),
        dense_weight,
        precision=lax.Precision.HIGHEST,
    )
    return placing.astype(jnp.bfloat16).reshape(ep_size * capacity, -1), slot_weight, capacity


def general_body(
    pool_input,
    pool_gain,
    mix_weight,
    moe_input,
    moe_gain,
    expert_ids,
    route_weight,
    gate_weight,
    up_weight,
    down_weight,
):
    pooled = pool_mixer(pool_input, pool_gain)
    ep_size = lax.axis_size("ep")
    out_columns = mix_weight.shape[1] // ep_size
    mix_columns = lax.dynamic_slice_in_dim(
        mix_weight, lax.axis_index("ep") * out_columns, out_columns, axis=1
    )
    mix_columns = lax.all_gather(mix_columns, "tp", axis=0, tiled=True)
    inputs = moe_input.astype(jnp.float32)
    scale_rows = lax.rsqrt(jnp.mean(inputs * inputs, axis=-1, keepdims=True) + eps_norm)
    normed = (inputs * scale_rows * moe_gain).astype(jnp.bfloat16)
    placing, slot_weight, capacity = dispatch_plan(expert_ids, route_weight, ep_size)
    rows = capacity // CHUNKS
    arrived_list = []
    placing_list = []
    for chunk in range(CHUNKS):
        chunk_placing = placing.reshape(ep_size, capacity, -1)[:, chunk * rows : (chunk + 1) * rows]
        chunk_placing = chunk_placing.reshape(ep_size * rows, -1)
        outgoing = jnp.dot(chunk_placing, normed, preferred_element_type=jnp.float32)
        outgoing = outgoing.astype(jnp.bfloat16)
        placing_list.append(chunk_placing)
        arrived_list.append(
            lax.all_to_all(outgoing, "ep", split_axis=0, concat_axis=0, tiled=True)
        )
    arrived_list[0], mix_columns = lax.optimization_barrier((arrived_list[0], mix_columns))
    weights = lax.all_to_all(slot_weight, "ep", split_axis=0, concat_axis=0, tiled=True)
    weights = lax.all_gather(weights, "tp", axis=0, tiled=True)
    combined = jnp.zeros(normed.shape, jnp.float32)
    for chunk in range(CHUNKS):
        tokens = lax.all_gather(arrived_list[chunk], "tp", axis=0, tiled=True)
        scales = weights[:, chunk * rows : (chunk + 1) * rows].reshape(tokens.shape[0], -1)
        gate_part = jnp.einsum(
            "nd,edf->enf", tokens, gate_weight, preferred_element_type=jnp.float32
        )
        upward = jnp.einsum("nd,edf->enf", tokens, up_weight, preferred_element_type=jnp.float32)
        hidden = (jax.nn.silu(gate_part) * upward * scales.T[:, :, None]).astype(jnp.bfloat16)
        partial = jnp.einsum("enf,edf->nd", hidden, down_weight, preferred_element_type=jnp.float32)
        reduced = lax.psum_scatter(
            partial.astype(jnp.bfloat16), "tp", scatter_dimension=0, tiled=True
        )
        returned = lax.all_to_all(reduced, "ep", split_axis=0, concat_axis=0, tiled=True)
        combined = combined + lax.dot_general(
            placing_list[chunk],
            returned,
            (((0,), (0,)), ((), ())),
            preferred_element_type=jnp.float32,
        )
    moe_out = combined.astype(jnp.bfloat16)
    regrouped = lax.all_to_all(pooled, "tp", split_axis=0, concat_axis=1, tiled=True)
    half = regrouped.shape[1] // 2
    mixed_sum = 0.0
    for part in range(2):
        section = slice(part * half, (part + 1) * half)
        pooled_rows = lax.all_gather(regrouped[:, section], "ep", axis=0, tiled=True)
        mixed_sum = mixed_sum + jnp.dot(
            pooled_rows, mix_columns[section], preferred_element_type=jnp.float32
        )
    mixed_out = lax.all_to_all(
        mixed_sum.astype(jnp.bfloat16), "ep", split_axis=0, concat_axis=1, tiled=True
    )
    return (mixed_out, moe_out)


LANES = 128
PIECES = 4
VMEM_LIMIT = 67043328
MESH = pl.DeviceIdType.MESH


def kernel_bytes(ep_size, planes, rows, slots, width, hidden, local_experts):
    wide = width + LANES
    block = ep_size * slots
    elements = planes * rows * wide
    elements += planes * (ep_size - 1) * slots * wide
    elements += planes * 2 * block * wide
    elements += 3 * local_experts * width * hidden
    elements += (planes * 2 + 4) * block * width
    elements += 2 * planes * rows * width
    elements += 2 * block * local_experts * hidden
    elements += rows * (wide + width)
    return 2 * elements


def expert_kernel(
    ep_size,
    planes,
    x_ref,
    gate_ref,
    up_ref,
    down_ref,
    out_ref,
    column,
    packed,
    tokens,
    gate_up,
    down,
    hidden,
    outgoing,
    partial,
    arriving,
    returned,
    running,
    weight_sems,
    line_send,
    line_recv,
    plane_send,
    plane_recv,
    share_send,
    share_recv,
    part_send,
    part_recv,
    back_send,
    back_recv,
    left_send,
    right_send,
    left_recv,
    right_recv,
):
    ep = lax.axis_index("ep")
    tp = lax.axis_index("tp")
    z = tp // 2
    core = tp % 2
    rows, wide = x_ref.shape
    local_experts, width, ff = gate_ref.shape
    slots = packed.shape[2]
    block = ep_size * slots
    piece = width // PIECES
    partner = (ep, tp + 1 - 2 * core)
    left = (ep, tp - 2)
    right = (ep, tp + 2)
    has_left = z > 0
    has_right = z < planes - 1
    at_end = (z * (planes - 1 - z)) == 0
    turn = 1 - 2 * (z // (planes // 2))

    inner = (z * (planes - 1 - z) + planes - 2) // (planes - 1)

    def source_of(step):
        both_ways = ((step + 1) // 2) * (2 * (step % 2) - 1)
        offset = inner * both_ways + (1 - inner) * step
        return (z + turn * offset + planes) % planes

    def sum_of(step):
        return (z + turn * step + planes) % planes

    def peer_of(offset):
        return ((ep + offset) % ep_size, tp)

    barrier = pltpu.get_barrier_semaphore()
    for offset in range(1, ep_size):
        pl.semaphore_signal(barrier, inc=1, device_id=peer_of(offset), device_id_type=MESH)
    pl.semaphore_signal(barrier, inc=1, device_id=partner, device_id_type=MESH)

    @pl.when(has_left)
    def _():
        pl.semaphore_signal(barrier, inc=1, device_id=left, device_id_type=MESH)

    @pl.when(has_right)
    def _():
        pl.semaphore_signal(barrier, inc=1, device_id=right, device_id_type=MESH)

    loads = []
    for expert in range(local_experts):
        lanes = pl.ds(expert * ff, ff)
        loads.append((gate_ref.at[expert], gate_up.at[expert, :, pl.ds(0, ff)]))
        loads.append((up_ref.at[expert], gate_up.at[expert, :, pl.ds(ff, ff)]))
        loads.append((down_ref.at[expert], down.at[:, lanes]))
    loads = [
        pltpu.make_async_copy(source, target, weight_sems.at[index])
        for index, (source, target) in enumerate(loads)
    ]
    for load in loads:
        load.start()

    pl.semaphore_wait(barrier, ep_size + 1 + inner)

    def line_copy(source_ref, source, direction):
        return pltpu.make_async_remote_copy(
            src_ref=source_ref,
            dst_ref=column.at[source],
            send_sem=line_send.at[source, direction],
            recv_sem=line_recv.at[source],
            device_id=(left, right)[direction],
            device_id_type=MESH,
        )

    def plane_copy(source, offset):
        return pltpu.make_async_remote_copy(
            src_ref=packed.at[source, offset - 1],
            dst_ref=tokens.at[source, core, pl.ds(pl.multiple_of(ep * slots, slots), slots)],
            send_sem=plane_send.at[source, offset - 1],
            recv_sem=plane_recv.at[source, offset - 1],
            device_id=peer_of(offset),
            device_id_type=MESH,
        )

    def share_copy(source):
        return pltpu.make_async_remote_copy(
            src_ref=tokens.at[source, core],
            dst_ref=tokens.at[source, core],
            send_sem=share_send.at[source],
            recv_sem=share_recv.at[source],
            device_id=partner,
            device_id_type=MESH,
        )

    def part_copy(source, slot, index):
        return pltpu.make_async_remote_copy(
            src_ref=outgoing.at[slot, index],
            dst_ref=arriving.at[slot, index],
            send_sem=part_send.at[slot, index],
            recv_sem=part_recv.at[slot, index],
            device_id=partner,
            device_id_type=MESH,
        )

    def back_copy(source, offset, index):
        target = (ep + offset) % ep_size
        return pltpu.make_async_remote_copy(
            src_ref=partial.at[source, index, pl.ds(pl.multiple_of(target * slots, slots), slots)],
            dst_ref=returned.at[source, index, pl.ds(pl.multiple_of(ep * slots, slots), slots)],
            send_sem=back_send.at[source, offset - 1, index],
            recv_sem=back_recv.at[source, offset - 1, index],
            device_id=(target, tp),
            device_id_type=MESH,
        )

    def sum_copy(source, index, direction):
        return pltpu.make_async_remote_copy(
            src_ref=running.at[1 - direction, source, index],
            dst_ref=running.at[1 - direction, source, index],
            send_sem=(left_send, right_send)[direction].at[source, index],
            recv_sem=(right_recv, left_recv)[direction].at[source, index],
            device_id=(left, right)[direction],
            device_id_type=MESH,
        )

    def dispatch(source_ref, source):
        routing = source_ref[:, width:].astype(jnp.float32).T
        for offset in range(ep_size):
            group = (ep + offset) % ep_size
            slot_row = jnp.zeros((1, rows), jnp.float32)
            for index in range(ep_size):
                row = 2 * local_experts + index
                chosen = jnp.where(index == group, 1.0, 0.0)
                slot_row = slot_row + routing[row : row + 1] * chosen
            places = lax.broadcasted_iota(jnp.int32, (slots, rows), 0).astype(jnp.float32)
            placing = jnp.where(places == slot_row, 1.0, 0.0).astype(jnp.bfloat16)
            compact = jnp.dot(placing, source_ref[...], preferred_element_type=jnp.float32)
            compact = compact.astype(jnp.bfloat16)
            if offset == 0:
                tokens[source, core, pl.ds(pl.multiple_of(ep * slots, slots), slots)] = compact
            else:
                packed[source, offset - 1] = compact
                plane_copy(source, offset).start()

    def gather(source):
        for offset in range(1, ep_size):
            plane_copy(source, offset).wait_recv()
        share_copy(source).start()

    def experts(source, slot):
        share_copy(source).wait_recv()

        def one(expert, carry):
            values = tokens[source].reshape(2 * block, wide)
            both = jnp.dot(
                values[:, :width], gate_up[expert], preferred_element_type=jnp.float32
            )
            lane = lax.broadcasted_iota(jnp.int32, (2 * block, LANES), 1)
            mine = (lane == expert) | (lane == local_experts + expert)
            scale = jnp.where(mine, values[:, width:].astype(jnp.float32), 0.0)
            scale = jnp.sum(scale, axis=1, keepdims=True)
            gated = both[:, :ff]
            gated = gated / (1.0 + jnp.exp(-gated))
            result = (gated * both[:, ff:] * scale).astype(jnp.bfloat16)
            hidden[:, pl.ds(pl.multiple_of(expert * ff, ff), ff)] = result
            return carry

        lax.fori_loop(0, local_experts, one, 0)

        def project(which, index):
            part = hidden[pl.ds(pl.multiple_of(which * block, block), block)]
            return lax.dot_general(
                part,
                down[index * piece : (index + 1) * piece],
                (((1,), (1,)), ((), ())),
                preferred_element_type=jnp.float32,
            )

        for index in range(PIECES):
            outgoing[slot, index] = project(1 - core, index).astype(jnp.bfloat16)
            part_copy(source, slot, index).start()
        for index in range(PIECES):
            own = project(core, index)
            part_copy(source, slot, index).wait_recv()
            total = own + arriving[slot, index].astype(jnp.float32)
            partial[source, index] = total.astype(jnp.bfloat16)
            own_rows = pl.ds(pl.multiple_of(ep * slots, slots), slots)
            returned[source, index, own_rows] = partial[source, index, own_rows]
            for offset in range(1, ep_size):
                back_copy(source, offset, index).start()

    def placing_back(source_ref):
        routing = source_ref[:, width:].astype(jnp.float32)
        pieces = []
        for group in range(ep_size):
            lane = 2 * local_experts + group
            places = lax.broadcasted_iota(jnp.int32, (rows, slots), 1).astype(jnp.float32)
            matched = places == routing[:, lane : lane + 1]
            pieces.append(jnp.where(matched, 1.0, 0.0))
        return jnp.concatenate(pieces, axis=1).astype(jnp.bfloat16)

    def combine(placing, source, index):
        for offset in range(1, ep_size):
            back_copy(source, offset, index).wait_recv()
        return jnp.dot(placing, returned[source, index], preferred_element_type=jnp.float32)

    def reduce_line(step):
        source = sum_of(step)
        placing = placing_back(column.at[source])
        for index in range(PIECES):
            mine = combine(placing, source, index)

            for direction in range(2):
                toward = (source < z, source > z)[direction]
                has_before = (has_right, has_left)[direction]

                @pl.when(toward & has_before)
                def _(direction=direction):
                    before = sum_copy(source, index, direction)
                    before.wait_recv()
                    total = mine + running[1 - direction, source, index].astype(jnp.float32)
                    running[1 - direction, source, index] = total.astype(jnp.bfloat16)
                    sum_copy(source, index, direction).start()

                @pl.when(toward & ~has_before)
                def _(direction=direction):
                    running[1 - direction, source, index] = mine.astype(jnp.bfloat16)
                    sum_copy(source, index, direction).start()

    @pl.when(has_left)
    def _():
        line_copy(x_ref, z, 0).start()

    @pl.when(has_right)
    def _():
        line_copy(x_ref, z, 1).start()

    dispatch(x_ref, z)
    for load in loads:
        load.wait()

    def step_body(step, carry):
        @pl.when(step < planes)
        def _():
            source = source_of(step)
            line_copy(x_ref, source, 0).wait_recv()

            @pl.when((source > z) & has_left)
            def _():
                line_copy(column.at[source], source, 0).start()

            @pl.when((source < z) & has_right)
            def _():
                line_copy(column.at[source], source, 1).start()

            dispatch(column.at[source], source)

        previous = source_of(step - 1)
        slot = (step - 1) % 2
        gather(previous)

        @pl.when(step > 2)
        def _():
            for index in range(PIECES):
                part_copy(previous, slot, index).wait_send()

        experts(previous, slot)

        @pl.when(at_end & (step > 2))
        def _():
            reduce_line(step - 2)

        return carry

    lax.fori_loop(1, planes + 1, step_body, 0)

    def tail_body(step, carry):
        @pl.when(~at_end | (step == planes - 1))
        def _():
            reduce_line(step)

        return carry

    lax.fori_loop(1, planes, tail_body, 0)

    placing = placing_back(x_ref)
    for index in range(PIECES):
        mine = combine(placing, z, index)
        lanes = pl.ds(index * piece, piece)

        for direction in range(2):
            has_before = (has_right, has_left)[direction]

            @pl.when(has_before)
            def _(direction=direction):
                sum_copy(z, index, direction).wait_recv()

        zero = jnp.zeros_like(mine)
        from_left = jnp.where(has_left, running[0, z, index].astype(jnp.float32), zero)
        from_right = jnp.where(has_right, running[1, z, index].astype(jnp.float32), zero)
        out_ref[:, lanes] = (mine + from_left + from_right).astype(jnp.bfloat16)

    @pl.when(has_left)
    def _():
        line_copy(x_ref, z, 0).wait_send()

    @pl.when(has_right)
    def _():
        line_copy(x_ref, z, 1).wait_send()

    def drain(source, carry):
        for offset in range(1, ep_size):
            plane_copy(source, offset).wait_send()
            for index in range(PIECES):
                back_copy(source, offset, index).wait_send()
        share_copy(source).wait_send()
        for direction in range(2):
            toward = (source < z, source > z)[direction]
            has_next = (has_left, has_right)[direction]
            forwarded = (source > z, source < z)[direction]

            @pl.when(toward)
            def _(direction=direction):
                for index in range(PIECES):
                    sum_copy(source, index, direction).wait_send()

            @pl.when(forwarded & has_next)
            def _(direction=direction):
                line_copy(x_ref, source, direction).wait_send()

        return carry

    lax.fori_loop(0, planes, drain, 0)
    for slot in range(2):
        for index in range(PIECES):
            part_copy(0, slot, index).wait_send()


def expert_layer(extended, gate_weight, up_weight, down_weight, ep_size, planes, slots):
    rows, wide = extended.shape
    local_experts, width, ff = gate_weight.shape
    block = ep_size * slots
    piece = width // PIECES
    half = jnp.bfloat16
    dma = pltpu.SemaphoreType.DMA
    return pl.pallas_call(
        functools.partial(expert_kernel, ep_size, planes),
        out_shape=jax.ShapeDtypeStruct((rows, width), half),
        in_specs=[pl.BlockSpec(memory_space=pltpu.VMEM)] + [pl.BlockSpec(memory_space=pl.ANY)] * 3,
        out_specs=pl.BlockSpec(memory_space=pltpu.VMEM),
        scratch_shapes=[
            pltpu.VMEM((planes, rows, wide), half),
            pltpu.VMEM((planes, ep_size - 1, slots, wide), half),
            pltpu.VMEM((planes, 2, block, wide), half),
            pltpu.VMEM((local_experts, width, 2 * ff), half),
            pltpu.VMEM((width, local_experts * ff), half),
            pltpu.VMEM((2 * block, local_experts * ff), half),
            pltpu.VMEM((2, PIECES, block, piece), half),
            pltpu.VMEM((planes, PIECES, block, piece), half),
            pltpu.VMEM((2, PIECES, block, piece), half),
            pltpu.VMEM((planes, PIECES, block, piece), half),
            pltpu.VMEM((2, planes, PIECES, rows, piece), half),
            dma((3 * local_experts,)),
            dma((planes, 2)),
            dma((planes,)),
            dma((planes, ep_size - 1)),
            dma((planes, ep_size - 1)),
            dma((planes,)),
            dma((planes,)),
            dma((2, PIECES)),
            dma((2, PIECES)),
            dma((planes, ep_size - 1, PIECES)),
            dma((planes, ep_size - 1, PIECES)),
            dma((planes, PIECES)),
            dma((planes, PIECES)),
            dma((planes, PIECES)),
            dma((planes, PIECES)),
        ],
        compiler_params=pltpu.CompilerParams(
            collective_id=0, has_side_effects=True, vmem_limit_bytes=VMEM_LIMIT
        ),
    )(extended, gate_weight, up_weight, down_weight)


def routing_lanes(expert_ids, route_weight, ep_size):
    local_experts = EXPERTS // ep_size
    owners = expert_ids // local_experts
    ep_index = lax.iota(jnp.int32, ep_size)
    member = jnp.any(owners[:, :, None] == ep_index[None, None, :], axis=1)
    counts = member.astype(jnp.int32)
    rank = jnp.cumsum(counts, axis=0) - counts
    slot = jnp.where(member, rank, -1).astype(jnp.float32)
    within = expert_ids % local_experts
    named = within[:, :, None] == lax.iota(jnp.int32, local_experts)[None, None, :]
    weights = jnp.sum(jnp.where(named, route_weight[:, :, None], 0.0), axis=1)
    high = lax.reduce_precision(weights, 8, 7)
    low = weights - high
    spare = LANES - 2 * local_experts - ep_size
    lanes = jnp.concatenate([high, low, slot], axis=1)
    return jnp.pad(lanes, ((0, 0), (0, spare))).astype(jnp.bfloat16)


def fast_body(
    pool_input,
    pool_gain,
    mix_weight,
    moe_input,
    moe_gain,
    expert_ids,
    route_weight,
    gate_weight,
    up_weight,
    down_weight,
):
    ep_size = lax.axis_size("ep")
    planes = lax.axis_size("tp") // 2
    local_experts = gate_weight.shape[0]
    slots = local_experts * CAP // TOP
    inputs = moe_input.astype(jnp.float32)
    scale_rows = lax.rsqrt(jnp.mean(inputs * inputs, axis=-1, keepdims=True) + eps_norm)
    normed = (inputs * scale_rows * moe_gain).astype(jnp.bfloat16)
    extended = jnp.concatenate([normed, routing_lanes(expert_ids, route_weight, ep_size)], axis=1)
    moe_out = expert_layer(
        extended, gate_weight, up_weight, down_weight, ep_size, planes, slots
    )
    pooled = pool_mixer(pool_input, pool_gain)
    mix_rows = lax.all_gather(mix_weight, "tp", axis=0, tiled=True)
    regrouped = lax.all_to_all(pooled, "tp", split_axis=0, concat_axis=1, tiled=True)
    mixed_out = jnp.dot(regrouped, mix_rows, preferred_element_type=jnp.float32)
    return (mixed_out.astype(jnp.bfloat16), moe_out)


def fits(mesh, shapes):
    moe_input, gate_weight = shapes
    ep_size = mesh.shape["ep"]
    tp_size = mesh.shape["tp"]
    experts, width, ff = gate_weight
    local_experts = experts // ep_size
    rows = moe_input[0] // (ep_size * tp_size)
    ff = ff // tp_size
    if local_experts % GROUP_EXP or tp_size % 4 or tp_size > 8 or ff % LANES or width % (PIECES * LANES):
        return False
    if 2 * local_experts + ep_size > LANES or rows > 256:
        return False
    slots = local_experts * CAP // TOP
    if slots % 16 or rows % 16:
        return False
    needed = kernel_bytes(ep_size, tp_size // 2, rows, slots, width, ff, local_experts)
    return needed < VMEM_LIMIT


def solution(mesh):
    def program(*arguments):
        shapes = (arguments[3].shape, arguments[7].shape)
        body = fast_body if fits(mesh, shapes) else general_body
        return jax.shard_map(
            body,
            mesh=mesh,
            in_specs=(
                P("ep", "tp"),
                P("tp"),
                P("tp", None),
                P(("ep", "tp"), None),
                P(),
                P(("ep", "tp"), None),
                P(("ep", "tp"), None),
                P("ep", None, "tp"),
                P("ep", None, "tp"),
                P("ep", None, "tp"),
            ),
            out_specs=(P(("ep", "tp"), None), P(("ep", "tp"), None)),
            check_vma=False,
        )(*arguments)

    return program
```

```python
import functools

import jax
import jax.numpy as jnp
from jax import lax
from jax.experimental import pallas as pl
from jax.experimental.pallas import tpu as pltpu
from jax.sharding import PartitionSpec as P

GROUP_CH = 256
EXPERTS = 16
GROUP_EXP = 4
TOP = 2
CAP = 48
CHUNKS = 2


eps_norm = 1e-06


def from_behind(shard, axis, by):
    peers = lax.axis_size(axis)
    pairs = [(i, i + by) for i in range(peers) if 0 <= i + by < peers]
    return lax.ppermute(shard, axis, pairs)


def window_sums(extended, row_count):
    level_sum = extended
    stride = 1
    outputs = []
    for doubling in range(4):
        level_sum = level_sum[stride:] + level_sum[:-stride]
        stride = stride * 2
        outputs.append(level_sum[level_sum.shape[0] - row_count :])
    return outputs


def pool_mixer(pool_input, pool_gain):
    row_count, channels = pool_input.shape
    carried = from_behind(pool_input[row_count - 15 :], "ep", 1)
    extended = jnp.concatenate([carried, pool_input], axis=0).astype(jnp.float32)
    window_list = window_sums(extended, row_count)
    channel_ids = lax.axis_index("tp") * channels + lax.iota(jnp.int32, channels)
    group_ids = channel_ids // GROUP_CH
    position = lax.axis_index("ep") * row_count + lax.iota(jnp.int32, row_count)
    summed = jnp.zeros((row_count, channels), jnp.float32)
    widths = jnp.zeros((channels,), jnp.int32)
    for index_group in range(4):
        inside = group_ids == index_group
        summed = jnp.where(inside[None, :], window_list[index_group], summed)
        widths = jnp.where(inside, 2 ** (index_group + 1), widths)
    counted = jnp.minimum(position[:, None] + 1, widths[None, :]).astype(jnp.float32)
    values = extended[15:]
    return ((summed / counted - values) * pool_gain).astype(jnp.bfloat16)


def dispatch_plan(expert_ids, route_weight, ep_size):
    local_experts = EXPERTS // ep_size
    share = TOP if local_experts % GROUP_EXP == 0 else 1
    capacity = local_experts * CAP // share
    owners = expert_ids // local_experts
    ep_index = lax.iota(jnp.int32, ep_size)
    member = jnp.any(owners[:, :, None] == ep_index[None, None, :], axis=1)
    counts = member.astype(jnp.int32)
    rank = jnp.cumsum(counts, axis=0) - counts
    slot = jnp.where(member, rank, -1).T
    placing = slot[:, None, :] == lax.iota(jnp.int32, capacity)[None, :, None]
    dense_weight = jnp.sum(
        jnp.where(
            expert_ids[:, :, None] == lax.iota(jnp.int32, EXPERTS)[None, None, :],
            route_weight[:, :, None],
            0.0,
        ),
        axis=1,
    )
    dense_weight = dense_weight.reshape(-1, ep_size, local_experts)
    slot_weight = jnp.einsum(
        "ecn,nej->ecj",
        placing.astype(jnp.float32),
        dense_weight,
        precision=lax.Precision.HIGHEST,
    )
    return placing.astype(jnp.bfloat16).reshape(ep_size * capacity, -1), slot_weight, capacity


def general_body(
    pool_input,
    pool_gain,
    mix_weight,
    moe_input,
    moe_gain,
    expert_ids,
    route_weight,
    gate_weight,
    up_weight,
    down_weight,
):
    pooled = pool_mixer(pool_input, pool_gain)
    ep_size = lax.axis_size("ep")
    out_columns = mix_weight.shape[1] // ep_size
    mix_columns = lax.dynamic_slice_in_dim(
        mix_weight, lax.axis_index("ep") * out_columns, out_columns, axis=1
    )
    mix_columns = lax.all_gather(mix_columns, "tp", axis=0, tiled=True)
    inputs = moe_input.astype(jnp.float32)
    scale_rows = lax.rsqrt(jnp.mean(inputs * inputs, axis=-1, keepdims=True) + eps_norm)
    normed = (inputs * scale_rows * moe_gain).astype(jnp.bfloat16)
    placing, slot_weight, capacity = dispatch_plan(expert_ids, route_weight, ep_size)
    rows = capacity // CHUNKS
    arrived_list = []
    placing_list = []
    for chunk in range(CHUNKS):
        chunk_placing = placing.reshape(ep_size, capacity, -1)[:, chunk * rows : (chunk + 1) * rows]
        chunk_placing = chunk_placing.reshape(ep_size * rows, -1)
        outgoing = jnp.dot(chunk_placing, normed, preferred_element_type=jnp.float32)
        outgoing = outgoing.astype(jnp.bfloat16)
        placing_list.append(chunk_placing)
        arrived_list.append(
            lax.all_to_all(outgoing, "ep", split_axis=0, concat_axis=0, tiled=True)
        )
    arrived_list[0], mix_columns = lax.optimization_barrier((arrived_list[0], mix_columns))
    weights = lax.all_to_all(slot_weight, "ep", split_axis=0, concat_axis=0, tiled=True)
    weights = lax.all_gather(weights, "tp", axis=0, tiled=True)
    combined = jnp.zeros(normed.shape, jnp.float32)
    for chunk in range(CHUNKS):
        tokens = lax.all_gather(arrived_list[chunk], "tp", axis=0, tiled=True)
        scales = weights[:, chunk * rows : (chunk + 1) * rows].reshape(tokens.shape[0], -1)
        gate_part = jnp.einsum(
            "nd,edf->enf", tokens, gate_weight, preferred_element_type=jnp.float32
        )
        upward = jnp.einsum("nd,edf->enf", tokens, up_weight, preferred_element_type=jnp.float32)
        hidden = (jax.nn.silu(gate_part) * upward * scales.T[:, :, None]).astype(jnp.bfloat16)
        partial = jnp.einsum("enf,edf->nd", hidden, down_weight, preferred_element_type=jnp.float32)
        reduced = lax.psum_scatter(
            partial.astype(jnp.bfloat16), "tp", scatter_dimension=0, tiled=True
        )
        returned = lax.all_to_all(reduced, "ep", split_axis=0, concat_axis=0, tiled=True)
        combined = combined + lax.dot_general(
            placing_list[chunk],
            returned,
            (((0,), (0,)), ((), ())),
            preferred_element_type=jnp.float32,
        )
    moe_out = combined.astype(jnp.bfloat16)
    regrouped = lax.all_to_all(pooled, "tp", split_axis=0, concat_axis=1, tiled=True)
    half = regrouped.shape[1] // 2
    mixed_sum = 0.0
    for part in range(2):
        section = slice(part * half, (part + 1) * half)
        pooled_rows = lax.all_gather(regrouped[:, section], "ep", axis=0, tiled=True)
        mixed_sum = mixed_sum + jnp.dot(
            pooled_rows, mix_columns[section], preferred_element_type=jnp.float32
        )
    mixed_out = lax.all_to_all(
        mixed_sum.astype(jnp.bfloat16), "ep", split_axis=0, concat_axis=1, tiled=True
    )
    return (mixed_out, moe_out)


LANES = 128
PIECES = 4
VMEM_LIMIT = 67043328
MESH = pl.DeviceIdType.MESH


def kernel_bytes(ep_size, planes, rows, slots, width, hidden, local_experts, mixer_elements):
    wide = width + LANES
    block = ep_size * slots
    elements = planes * rows * wide
    elements += planes * (ep_size - 1) * slots * wide
    elements += planes * 2 * block * wide
    elements += 3 * local_experts * width * hidden
    elements += (planes * 2 + 4) * block * width
    elements += (planes + 1) * rows * width
    elements += 2 * block * local_experts * hidden
    elements += rows * (wide + width)
    elements += mixer_elements
    return 2 * elements


def expert_kernel(
    ep_size,
    planes,
    x_ref,
    pool_ref,
    gain_ref,
    mix_ref,
    gate_ref,
    up_ref,
    down_ref,
    mixed_ref,
    out_ref,
    column,
    packed,
    tokens,
    gate_up,
    down,
    hidden,
    outgoing,
    partial,
    arriving,
    returned,
    running,
    weight_sems,
    line_send,
    line_recv,
    plane_send,
    plane_recv,
    share_send,
    share_recv,
    part_send,
    part_recv,
    back_send,
    back_recv,
    left_send,
    right_send,
    left_recv,
    right_recv,
    halo,
    pooled,
    regrouped,
    mix,
    halo_sems,
    mix_load,
    pool_send,
    pool_recv,
    mix_send,
    mix_recv,
    pair_send,
    pair_recv,
):
    ep = lax.axis_index("ep")
    tp = lax.axis_index("tp")
    z = tp // 2
    core = tp % 2
    rows, wide = x_ref.shape
    local_experts, width, ff = gate_ref.shape
    slots = packed.shape[2]
    block = ep_size * slots
    piece = width // PIECES
    partner = (ep, tp + 1 - 2 * core)
    left = (ep, tp - 2)
    right = (ep, tp + 2)
    has_left = z > 0
    has_right = z < planes - 1
    at_end = (z * (planes - 1 - z)) == 0
    turn = 1 - 2 * (z // (planes // 2))

    inner = (z * (planes - 1 - z) + planes - 2) // (planes - 1)

    def source_of(step):
        both_ways = ((step + 1) // 2) * (2 * (step % 2) - 1)
        offset = inner * both_ways + (1 - inner) * step
        return (z + turn * offset + planes) % planes

    def sum_of(step):
        return (z + turn * step + planes) % planes

    def peer_of(offset):
        return ((ep + offset) % ep_size, tp)

    tp_size = 2 * planes
    barrier = pltpu.get_barrier_semaphore()
    for offset in range(1, ep_size):
        pl.semaphore_signal(barrier, inc=1, device_id=peer_of(offset), device_id_type=MESH)
    for offset in range(1, tp_size):
        pl.semaphore_signal(
            barrier, inc=1, device_id=(ep, (tp + offset) % tp_size), device_id_type=MESH
        )

    loads = []
    for expert in range(local_experts):
        lanes = pl.ds(expert * ff, ff)
        loads.append((gate_ref.at[expert], gate_up.at[expert, :, pl.ds(0, ff)]))
        loads.append((up_ref.at[expert], gate_up.at[expert, :, pl.ds(ff, ff)]))
        loads.append((down_ref.at[expert], down.at[:, lanes]))
    loads = [
        pltpu.make_async_copy(source, target, weight_sems.at[index])
        for index, (source, target) in enumerate(loads)
    ]
    for load in loads:
        load.start()
    mix_own = pltpu.make_async_copy(mix_ref, mix.at[tp], mix_load)
    mix_own.start()
    pl.semaphore_wait(barrier, ep_size + tp_size - 2)

    def line_copy(source_ref, source, direction):
        return pltpu.make_async_remote_copy(
            src_ref=source_ref,
            dst_ref=column.at[source],
            send_sem=line_send.at[source, direction],
            recv_sem=line_recv.at[source],
            device_id=(left, right)[direction],
            device_id_type=MESH,
        )

    def plane_copy(source, offset):
        return pltpu.make_async_remote_copy(
            src_ref=packed.at[source, offset - 1],
            dst_ref=tokens.at[source, core, pl.ds(pl.multiple_of(ep * slots, slots), slots)],
            send_sem=plane_send.at[source, offset - 1],
            recv_sem=plane_recv.at[source, offset - 1],
            device_id=peer_of(offset),
            device_id_type=MESH,
        )

    def share_copy(source):
        return pltpu.make_async_remote_copy(
            src_ref=tokens.at[source, core],
            dst_ref=tokens.at[source, core],
            send_sem=share_send.at[source],
            recv_sem=share_recv.at[source],
            device_id=partner,
            device_id_type=MESH,
        )

    def part_copy(source, slot, index):
        return pltpu.make_async_remote_copy(
            src_ref=outgoing.at[slot, index],
            dst_ref=arriving.at[slot, index],
            send_sem=part_send.at[slot, index],
            recv_sem=part_recv.at[slot, index],
            device_id=partner,
            device_id_type=MESH,
        )

    def back_copy(source, offset, index):
        target = (ep + offset) % ep_size
        return pltpu.make_async_remote_copy(
            src_ref=partial.at[source, index, pl.ds(pl.multiple_of(target * slots, slots), slots)],
            dst_ref=returned.at[source, index, pl.ds(pl.multiple_of(ep * slots, slots), slots)],
            send_sem=back_send.at[source, offset - 1, index],
            recv_sem=back_recv.at[source, offset - 1, index],
            device_id=(target, tp),
            device_id_type=MESH,
        )

    def sum_copy(source, place, index, direction):
        return pltpu.make_async_remote_copy(
            src_ref=running.at[source, index],
            dst_ref=running.at[place, index],
            send_sem=(left_send, right_send)[direction].at[source, index],
            recv_sem=(right_recv, left_recv)[direction].at[source, index],
            device_id=(left, right)[direction],
            device_id_type=MESH,
        )

    def sum_place(source, direction):
        if direction == 1:
            return source
        ends = (source + 1) // jnp.maximum(z, 1)
        return source + (planes - source) * ends

    sequence, channels = pool_ref.shape
    share_rows = sequence // tp_size
    edge = halo.shape[0]

    def halo_copy():
        return pltpu.make_async_remote_copy(
            src_ref=pool_ref.at[pl.ds(sequence - edge, edge)],
            dst_ref=halo,
            send_sem=halo_sems.at[0],
            recv_sem=halo_sems.at[1],
            device_id=peer_of(1),
            device_id_type=MESH,
        )

    def pool_copy(offset):
        target = (tp + offset) % tp_size
        lanes = pl.ds(pl.multiple_of(tp * channels, channels), channels)
        return pltpu.make_async_remote_copy(
            src_ref=pooled.at[pl.ds(pl.multiple_of(target * share_rows, share_rows), share_rows)],
            dst_ref=regrouped.at[:, lanes],
            send_sem=pool_send.at[offset - 1],
            recv_sem=pool_recv.at[offset - 1],
            device_id=(ep, target),
            device_id_type=MESH,
        )

    def mix_copy(offset):
        return pltpu.make_async_remote_copy(
            src_ref=mix.at[tp],
            dst_ref=mix.at[tp],
            send_sem=mix_send.at[offset - 1],
            recv_sem=mix_recv.at[offset - 1],
            device_id=(ep, (tp + 2 * offset) % tp_size),
            device_id_type=MESH,
        )

    def pair_copy(offset):
        block_of = (tp - 2 * offset + tp_size) % tp_size
        return pltpu.make_async_remote_copy(
            src_ref=mix.at[block_of],
            dst_ref=mix.at[block_of],
            send_sem=pair_send.at[offset],
            recv_sem=pair_recv.at[offset],
            device_id=partner,
            device_id_type=MESH,
        )

    def pool():
        @pl.when(ep > 0)
        def _():
            halo_copy().wait_recv()

        before = jnp.where(ep > 0, halo[...].astype(jnp.float32), 0.0)
        values = pool_ref[...].astype(jnp.float32)
        level = jnp.concatenate([before, values], axis=0)
        channel = tp * channels + lax.broadcasted_iota(jnp.int32, (1, channels), 1)
        position = ep * sequence + lax.broadcasted_iota(jnp.int32, (sequence, 1), 0)
        summed = jnp.zeros((sequence, channels), jnp.float32)
        widths = jnp.zeros((1, channels), jnp.int32)
        for index in range(4):
            level = level + pltpu.roll(level, 2**index, 0)
            inside = (channel >= index * GROUP_CH) & (channel < (index + 1) * GROUP_CH)
            summed = jnp.where(inside, level[edge:], summed)
            widths = jnp.where(inside, 2 ** (index + 1), widths)
        counted = jnp.minimum(position + 1, widths).astype(jnp.float32)
        result = (summed / counted - values) * gain_ref[...]
        pooled[...] = result.astype(jnp.bfloat16)
        own_rows = pl.ds(pl.multiple_of(tp * share_rows, share_rows), share_rows)
        lanes = pl.ds(pl.multiple_of(tp * channels, channels), channels)
        regrouped[:, lanes] = pooled[own_rows]

    def send_mixer():
        mix_own.wait()
        for offset in range(1, tp_size):
            pool_copy(offset).start()
        for offset in range(1, planes):
            mix_copy(offset).start()
        pair_copy(0).start()

    def pair_mixer():
        for offset in range(1, planes):
            mix_copy(offset).wait_recv()
            pair_copy(offset).start()

    def mixer():
        for offset in range(1, tp_size):
            pool_copy(offset).wait_recv()
        for offset in range(planes):
            pair_copy(offset).wait_recv()
        total = jnp.zeros((share_rows, mix.shape[2]), jnp.float32)
        for index in range(tp_size):
            part = regrouped[:, index * channels : (index + 1) * channels]
            total = total + jnp.dot(part, mix[index], preferred_element_type=jnp.float32)
        mixed_ref[...] = total.astype(jnp.bfloat16)

    def dispatch(source_ref, source):
        routing = source_ref[:, width:].astype(jnp.float32).T
        for offset in range(ep_size):
            group = (ep + offset) % ep_size
            slot_row = jnp.zeros((1, rows), jnp.float32)
            for index in range(ep_size):
                row = 2 * local_experts + index
                chosen = jnp.where(index == group, 1.0, 0.0)
                slot_row = slot_row + routing[row : row + 1] * chosen
            places = lax.broadcasted_iota(jnp.int32, (slots, rows), 0).astype(jnp.float32)
            placing = jnp.where(places == slot_row, 1.0, 0.0).astype(jnp.bfloat16)
            compact = jnp.dot(placing, source_ref[...], preferred_element_type=jnp.float32)
            compact = compact.astype(jnp.bfloat16)
            if offset == 0:
                tokens[source, core, pl.ds(pl.multiple_of(ep * slots, slots), slots)] = compact
            else:
                packed[source, offset - 1] = compact
                plane_copy(source, offset).start()

    def gather(source):
        for offset in range(1, ep_size):
            plane_copy(source, offset).wait_recv()
        share_copy(source).start()

    def experts(source, slot):
        share_copy(source).wait_recv()

        def one(expert, carry):
            values = tokens[source].reshape(2 * block, wide)
            both = jnp.dot(
                values[:, :width], gate_up[expert], preferred_element_type=jnp.float32
            )
            lane = lax.broadcasted_iota(jnp.int32, (2 * block, LANES), 1)
            mine = (lane == expert) | (lane == local_experts + expert)
            scale = jnp.where(mine, values[:, width:].astype(jnp.float32), 0.0)
            scale = jnp.sum(scale, axis=1, keepdims=True)
            gated = both[:, :ff]
            gated = gated / (1.0 + jnp.exp(-gated))
            result = (gated * both[:, ff:] * scale).astype(jnp.bfloat16)
            hidden[:, pl.ds(pl.multiple_of(expert * ff, ff), ff)] = result
            return carry

        lax.fori_loop(0, local_experts, one, 0)

        def project(which, index):
            part = hidden[pl.ds(pl.multiple_of(which * block, block), block)]
            return lax.dot_general(
                part,
                down[index * piece : (index + 1) * piece],
                (((1,), (1,)), ((), ())),
                preferred_element_type=jnp.float32,
            )

        for index in range(PIECES):
            outgoing[slot, index] = project(1 - core, index).astype(jnp.bfloat16)
            part_copy(source, slot, index).start()
        for index in range(PIECES):
            own = project(core, index)
            part_copy(source, slot, index).wait_recv()
            total = own + arriving[slot, index].astype(jnp.float32)
            partial[source, index] = total.astype(jnp.bfloat16)
            own_rows = pl.ds(pl.multiple_of(ep * slots, slots), slots)
            returned[source, index, own_rows] = partial[source, index, own_rows]
            for offset in range(1, ep_size):
                back_copy(source, offset, index).start()

    def placing_back(source_ref):
        routing = source_ref[:, width:].astype(jnp.float32)
        pieces = []
        for group in range(ep_size):
            lane = 2 * local_experts + group
            places = lax.broadcasted_iota(jnp.int32, (rows, slots), 1).astype(jnp.float32)
            matched = places == routing[:, lane : lane + 1]
            pieces.append(jnp.where(matched, 1.0, 0.0))
        return jnp.concatenate(pieces, axis=1).astype(jnp.bfloat16)

    def combine(placing, source, index):
        for offset in range(1, ep_size):
            back_copy(source, offset, index).wait_recv()
        return jnp.dot(placing, returned[source, index], preferred_element_type=jnp.float32)

    def reduce_line(step):
        source = sum_of(step)
        placing = placing_back(column.at[source])
        for index in range(PIECES):
            mine = combine(placing, source, index)

            for direction in range(2):
                toward = (source < z, source > z)[direction]
                has_before = (has_right, has_left)[direction]

                @pl.when(toward & has_before)
                def _(direction=direction):
                    sum_copy(source, source, index, direction).wait_recv()
                    total = mine + running[source, index].astype(jnp.float32)
                    running[source, index] = total.astype(jnp.bfloat16)
                    place = sum_place(source, direction)
                    sum_copy(source, place, index, direction).start()

                @pl.when(toward & ~has_before)
                def _(direction=direction):
                    running[source, index] = mine.astype(jnp.bfloat16)
                    place = sum_place(source, direction)
                    sum_copy(source, place, index, direction).start()

    @pl.when(has_left)
    def _():
        line_copy(x_ref, z, 0).start()

    @pl.when(has_right)
    def _():
        line_copy(x_ref, z, 1).start()

    @pl.when(ep < ep_size - 1)
    def _():
        halo_copy().start()

    dispatch(x_ref, z)
    pool()
    for load in loads:
        load.wait()

    def step_body(step, carry):
        @pl.when(step < planes)
        def _():
            source = source_of(step)
            line_copy(x_ref, source, 0).wait_recv()

            @pl.when((source > z) & has_left)
            def _():
                line_copy(column.at[source], source, 0).start()

            @pl.when((source < z) & has_right)
            def _():
                line_copy(column.at[source], source, 1).start()

            dispatch(column.at[source], source)

        @pl.when(step == planes - 1)
        def _():
            send_mixer()

        previous = source_of(step - 1)
        slot = (step - 1) % 2
        gather(previous)

        @pl.when(step > 2)
        def _():
            for index in range(PIECES):
                part_copy(previous, slot, index).wait_send()

        experts(previous, slot)

        @pl.when(at_end & (step > 2))
        def _():
            reduce_line(step - 2)

        return carry

    lax.fori_loop(1, planes + 1, step_body, 0)
    pair_mixer()

    def tail_body(step, carry):
        @pl.when(~at_end | (step == planes - 1))
        def _():
            reduce_line(step)

        return carry

    lax.fori_loop(1, planes, tail_body, 0)
    mixer()

    placing = placing_back(x_ref)
    for index in range(PIECES):
        mine = combine(placing, z, index)
        lanes = pl.ds(index * piece, piece)

        for direction in range(2):
            has_before = (has_right, has_left)[direction]

            @pl.when(has_before)
            def _(direction=direction):
                sum_copy(z, z, index, direction).wait_recv()

        zero = jnp.zeros_like(mine)
        from_left = jnp.where(has_left, running[z, index].astype(jnp.float32), zero)
        from_right = jnp.where(has_right, running[planes, index].astype(jnp.float32), zero)
        out_ref[:, lanes] = (mine + from_left + from_right).astype(jnp.bfloat16)

    @pl.when(has_left)
    def _():
        line_copy(x_ref, z, 0).wait_send()

    @pl.when(has_right)
    def _():
        line_copy(x_ref, z, 1).wait_send()

    @pl.when(ep < ep_size - 1)
    def _():
        halo_copy().wait_send()

    for offset in range(1, tp_size):
        pool_copy(offset).wait_send()
    for offset in range(1, planes):
        mix_copy(offset).wait_send()
    for offset in range(planes):
        pair_copy(offset).wait_send()

    def drain(source, carry):
        for offset in range(1, ep_size):
            plane_copy(source, offset).wait_send()
            for index in range(PIECES):
                back_copy(source, offset, index).wait_send()
        share_copy(source).wait_send()
        for direction in range(2):
            toward = (source < z, source > z)[direction]
            has_next = (has_left, has_right)[direction]
            forwarded = (source > z, source < z)[direction]

            @pl.when(toward)
            def _(direction=direction):
                for index in range(PIECES):
                    sum_copy(source, source, index, direction).wait_send()

            @pl.when(forwarded & has_next)
            def _(direction=direction):
                line_copy(x_ref, source, direction).wait_send()

        return carry

    lax.fori_loop(0, planes, drain, 0)
    for slot in range(2):
        for index in range(PIECES):
            part_copy(0, slot, index).wait_send()


def fused_layers(extended, pool_input, pool_gain, mix_weight, weights, ep_size, planes, slots):
    gate_weight, up_weight, down_weight = weights
    rows, wide = extended.shape
    sequence, channels = pool_input.shape
    depth, outputs = mix_weight.shape
    tp_size = 2 * planes
    share_rows = sequence // tp_size
    edge = 16
    local_experts, width, ff = gate_weight.shape
    block = ep_size * slots
    piece = width // PIECES
    half = jnp.bfloat16
    dma = pltpu.SemaphoreType.DMA
    return pl.pallas_call(
        functools.partial(expert_kernel, ep_size, planes),
        out_shape=(
            jax.ShapeDtypeStruct((share_rows, outputs), half),
            jax.ShapeDtypeStruct((rows, width), half),
        ),
        in_specs=[pl.BlockSpec(memory_space=pltpu.VMEM)] * 3
        + [pl.BlockSpec(memory_space=pl.ANY)] * 4,
        out_specs=(pl.BlockSpec(memory_space=pltpu.VMEM),) * 2,
        scratch_shapes=[
            pltpu.VMEM((planes, rows, wide), half),
            pltpu.VMEM((planes, ep_size - 1, slots, wide), half),
            pltpu.VMEM((planes, 2, block, wide), half),
            pltpu.VMEM((local_experts, width, 2 * ff), half),
            pltpu.VMEM((width, local_experts * ff), half),
            pltpu.VMEM((2 * block, local_experts * ff), half),
            pltpu.VMEM((2, PIECES, block, piece), half),
            pltpu.VMEM((planes, PIECES, block, piece), half),
            pltpu.VMEM((2, PIECES, block, piece), half),
            pltpu.VMEM((planes, PIECES, block, piece), half),
            pltpu.VMEM((planes + 1, PIECES, rows, piece), half),
            dma((3 * local_experts,)),
            dma((planes, 2)),
            dma((planes,)),
            dma((planes, ep_size - 1)),
            dma((planes, ep_size - 1)),
            dma((planes,)),
            dma((planes,)),
            dma((2, PIECES)),
            dma((2, PIECES)),
            dma((planes, ep_size - 1, PIECES)),
            dma((planes, ep_size - 1, PIECES)),
            dma((planes, PIECES)),
            dma((planes, PIECES)),
            dma((planes, PIECES)),
            dma((planes, PIECES)),
            pltpu.VMEM((edge, channels), half),
            pltpu.VMEM((sequence, channels), half),
            pltpu.VMEM((share_rows, tp_size * channels), half),
            pltpu.VMEM((tp_size, depth, outputs), half),
            dma((2,)),
            dma,
            dma((tp_size - 1,)),
            dma((tp_size - 1,)),
            dma((planes - 1,)),
            dma((planes - 1,)),
            dma((planes,)),
            dma((planes,)),
        ],
        compiler_params=pltpu.CompilerParams(
            collective_id=0, has_side_effects=True, vmem_limit_bytes=VMEM_LIMIT
        ),
    )(extended, pool_input, pool_gain[None, :], mix_weight, gate_weight, up_weight, down_weight)


def routing_lanes(expert_ids, route_weight, ep_size):
    local_experts = EXPERTS // ep_size
    owners = expert_ids // local_experts
    ep_index = lax.iota(jnp.int32, ep_size)
    member = jnp.any(owners[:, :, None] == ep_index[None, None, :], axis=1)
    counts = member.astype(jnp.int32)
    rank = jnp.cumsum(counts, axis=0) - counts
    slot = jnp.where(member, rank, -1).astype(jnp.float32)
    within = expert_ids % local_experts
    named = within[:, :, None] == lax.iota(jnp.int32, local_experts)[None, None, :]
    weights = jnp.sum(jnp.where(named, route_weight[:, :, None], 0.0), axis=1)
    high = lax.reduce_precision(weights, 8, 7)
    low = weights - high
    spare = LANES - 2 * local_experts - ep_size
    lanes = jnp.concatenate([high, low, slot], axis=1)
    return jnp.pad(lanes, ((0, 0), (0, spare))).astype(jnp.bfloat16)


def fast_body(
    pool_input,
    pool_gain,
    mix_weight,
    moe_input,
    moe_gain,
    expert_ids,
    route_weight,
    gate_weight,
    up_weight,
    down_weight,
):
    ep_size = lax.axis_size("ep")
    planes = lax.axis_size("tp") // 2
    local_experts = gate_weight.shape[0]
    slots = local_experts * CAP // TOP
    inputs = moe_input.astype(jnp.float32)
    scale_rows = lax.rsqrt(jnp.mean(inputs * inputs, axis=-1, keepdims=True) + eps_norm)
    normed = (inputs * scale_rows * moe_gain).astype(jnp.bfloat16)
    extended = jnp.concatenate([normed, routing_lanes(expert_ids, route_weight, ep_size)], axis=1)
    return fused_layers(
        extended,
        pool_input,
        pool_gain,
        mix_weight,
        (gate_weight, up_weight, down_weight),
        ep_size,
        planes,
        slots,
    )


def fits(mesh, shapes):
    pool_input, mix_weight, moe_input, gate_weight = shapes
    ep_size = mesh.shape["ep"]
    tp_size = mesh.shape["tp"]
    experts, width, ff = gate_weight
    local_experts = experts // ep_size
    rows = moe_input[0] // (ep_size * tp_size)
    ff = ff // tp_size
    if local_experts % GROUP_EXP or tp_size % 4 or tp_size > 8 or ff % LANES or width % (PIECES * LANES):
        return False
    if 2 * local_experts + ep_size > LANES or rows > 256:
        return False
    slots = local_experts * CAP // TOP
    if slots % 16 or rows % 16:
        return False
    sequence = pool_input[0] // ep_size
    channels = pool_input[1] // tp_size
    share_rows = sequence // tp_size
    if channels % LANES or mix_weight[0] != pool_input[1] or share_rows % 16 or mix_weight[1] % LANES:
        return False
    mixer = mix_weight[0] * mix_weight[1] + share_rows * (mix_weight[0] + mix_weight[1])
    mixer += 2 * sequence * channels
    needed = kernel_bytes(ep_size, tp_size // 2, rows, slots, width, ff, local_experts, mixer)
    return needed < VMEM_LIMIT


def solution(mesh):
    def program(*arguments):
        shapes = tuple(arguments[index].shape for index in (0, 2, 3, 7))
        body = fast_body if fits(mesh, shapes) else general_body
        return jax.shard_map(
            body,
            mesh=mesh,
            in_specs=(
                P("ep", "tp"),
                P("tp"),
                P("tp", None),
                P(("ep", "tp"), None),
                P(),
                P(("ep", "tp"), None),
                P(("ep", "tp"), None),
                P("ep", None, "tp"),
                P("ep", None, "tp"),
                P("ep", None, "tp"),
            ),
            out_specs=(P(("ep", "tp"), None), P(("ep", "tp"), None)),
            check_vma=False,
        )(*arguments)

    return program
```

```python
import functools

import jax
import jax.numpy as jnp
from jax import lax
from jax.experimental import pallas as pl
from jax.experimental.pallas import tpu as pltpu
from jax.sharding import PartitionSpec as P

GROUP_CH = 256
EXPERTS = 16
GROUP_EXP = 4
TOP = 2
CAP = 48
CHUNKS = 2


eps_norm = 1e-06


def from_behind(shard, axis, by):
    peers = lax.axis_size(axis)
    pairs = [(i, i + by) for i in range(peers) if 0 <= i + by < peers]
    return lax.ppermute(shard, axis, pairs)


def window_sums(extended, row_count):
    level_sum = extended
    stride = 1
    outputs = []
    for doubling in range(4):
        level_sum = level_sum[stride:] + level_sum[:-stride]
        stride = stride * 2
        outputs.append(level_sum[level_sum.shape[0] - row_count :])
    return outputs


def pool_mixer(pool_input, pool_gain):
    row_count, channels = pool_input.shape
    carried = from_behind(pool_input[row_count - 15 :], "ep", 1)
    extended = jnp.concatenate([carried, pool_input], axis=0).astype(jnp.float32)
    window_list = window_sums(extended, row_count)
    channel_ids = lax.axis_index("tp") * channels + lax.iota(jnp.int32, channels)
    group_ids = channel_ids // GROUP_CH
    position = lax.axis_index("ep") * row_count + lax.iota(jnp.int32, row_count)
    summed = jnp.zeros((row_count, channels), jnp.float32)
    widths = jnp.zeros((channels,), jnp.int32)
    for index_group in range(4):
        inside = group_ids == index_group
        summed = jnp.where(inside[None, :], window_list[index_group], summed)
        widths = jnp.where(inside, 2 ** (index_group + 1), widths)
    counted = jnp.minimum(position[:, None] + 1, widths[None, :]).astype(jnp.float32)
    values = extended[15:]
    return ((summed / counted - values) * pool_gain).astype(jnp.bfloat16)


def dispatch_plan(expert_ids, route_weight, ep_size):
    local_experts = EXPERTS // ep_size
    share = TOP if local_experts % GROUP_EXP == 0 else 1
    capacity = local_experts * CAP // share
    owners = expert_ids // local_experts
    ep_index = lax.iota(jnp.int32, ep_size)
    member = jnp.any(owners[:, :, None] == ep_index[None, None, :], axis=1)
    counts = member.astype(jnp.int32)
    rank = jnp.cumsum(counts, axis=0) - counts
    slot = jnp.where(member, rank, -1).T
    placing = slot[:, None, :] == lax.iota(jnp.int32, capacity)[None, :, None]
    dense_weight = jnp.sum(
        jnp.where(
            expert_ids[:, :, None] == lax.iota(jnp.int32, EXPERTS)[None, None, :],
            route_weight[:, :, None],
            0.0,
        ),
        axis=1,
    )
    dense_weight = dense_weight.reshape(-1, ep_size, local_experts)
    slot_weight = jnp.einsum(
        "ecn,nej->ecj",
        placing.astype(jnp.float32),
        dense_weight,
        precision=lax.Precision.HIGHEST,
    )
    return placing.astype(jnp.bfloat16).reshape(ep_size * capacity, -1), slot_weight, capacity


def general_body(
    pool_input,
    pool_gain,
    mix_weight,
    moe_input,
    moe_gain,
    expert_ids,
    route_weight,
    gate_weight,
    up_weight,
    down_weight,
):
    pooled = pool_mixer(pool_input, pool_gain)
    ep_size = lax.axis_size("ep")
    out_columns = mix_weight.shape[1] // ep_size
    mix_columns = lax.dynamic_slice_in_dim(
        mix_weight, lax.axis_index("ep") * out_columns, out_columns, axis=1
    )
    mix_columns = lax.all_gather(mix_columns, "tp", axis=0, tiled=True)
    inputs = moe_input.astype(jnp.float32)
    scale_rows = lax.rsqrt(jnp.mean(inputs * inputs, axis=-1, keepdims=True) + eps_norm)
    normed = (inputs * scale_rows * moe_gain).astype(jnp.bfloat16)
    placing, slot_weight, capacity = dispatch_plan(expert_ids, route_weight, ep_size)
    rows = capacity // CHUNKS
    arrived_list = []
    placing_list = []
    for chunk in range(CHUNKS):
        chunk_placing = placing.reshape(ep_size, capacity, -1)[:, chunk * rows : (chunk + 1) * rows]
        chunk_placing = chunk_placing.reshape(ep_size * rows, -1)
        outgoing = jnp.dot(chunk_placing, normed, preferred_element_type=jnp.float32)
        outgoing = outgoing.astype(jnp.bfloat16)
        placing_list.append(chunk_placing)
        arrived_list.append(
            lax.all_to_all(outgoing, "ep", split_axis=0, concat_axis=0, tiled=True)
        )
    arrived_list[0], mix_columns = lax.optimization_barrier((arrived_list[0], mix_columns))
    weights = lax.all_to_all(slot_weight, "ep", split_axis=0, concat_axis=0, tiled=True)
    weights = lax.all_gather(weights, "tp", axis=0, tiled=True)
    combined = jnp.zeros(normed.shape, jnp.float32)
    for chunk in range(CHUNKS):
        tokens = lax.all_gather(arrived_list[chunk], "tp", axis=0, tiled=True)
        scales = weights[:, chunk * rows : (chunk + 1) * rows].reshape(tokens.shape[0], -1)
        gate_part = jnp.einsum(
            "nd,edf->enf", tokens, gate_weight, preferred_element_type=jnp.float32
        )
        upward = jnp.einsum("nd,edf->enf", tokens, up_weight, preferred_element_type=jnp.float32)
        hidden = (jax.nn.silu(gate_part) * upward * scales.T[:, :, None]).astype(jnp.bfloat16)
        partial = jnp.einsum("enf,edf->nd", hidden, down_weight, preferred_element_type=jnp.float32)
        reduced = lax.psum_scatter(
            partial.astype(jnp.bfloat16), "tp", scatter_dimension=0, tiled=True
        )
        returned = lax.all_to_all(reduced, "ep", split_axis=0, concat_axis=0, tiled=True)
        combined = combined + lax.dot_general(
            placing_list[chunk],
            returned,
            (((0,), (0,)), ((), ())),
            preferred_element_type=jnp.float32,
        )
    moe_out = combined.astype(jnp.bfloat16)
    regrouped = lax.all_to_all(pooled, "tp", split_axis=0, concat_axis=1, tiled=True)
    half = regrouped.shape[1] // 2
    mixed_sum = 0.0
    for part in range(2):
        section = slice(part * half, (part + 1) * half)
        pooled_rows = lax.all_gather(regrouped[:, section], "ep", axis=0, tiled=True)
        mixed_sum = mixed_sum + jnp.dot(
            pooled_rows, mix_columns[section], preferred_element_type=jnp.float32
        )
    mixed_out = lax.all_to_all(
        mixed_sum.astype(jnp.bfloat16), "ep", split_axis=0, concat_axis=1, tiled=True
    )
    return (mixed_out, moe_out)


LANES = 128
PIECES = 4
VMEM_LIMIT = 67043328
MESH = pl.DeviceIdType.MESH


def kernel_bytes(ep_size, planes, rows, slots, width, hidden, local_experts, mixer_elements):
    wide = width + LANES
    block = ep_size * slots
    elements = planes * rows * wide
    elements += planes * (ep_size - 1) * slots * wide
    elements += planes * 2 * block * wide
    elements += 3 * local_experts * width * hidden
    elements += (planes * 2 + 4) * block * width
    elements += (planes + 1) * rows * width
    elements += 2 * block * local_experts * hidden
    elements += rows * (wide + width)
    elements += mixer_elements
    return 2 * elements


def expert_kernel(
    ep_size,
    planes,
    x_ref,
    pool_ref,
    gain_ref,
    mix_ref,
    gate_ref,
    up_ref,
    down_ref,
    mixed_ref,
    out_ref,
    column,
    packed,
    tokens,
    gate_up,
    down,
    hidden,
    outgoing,
    partial,
    arriving,
    returned,
    running,
    weight_sems,
    line_send,
    line_recv,
    plane_send,
    plane_recv,
    share_send,
    share_recv,
    part_send,
    part_recv,
    back_send,
    back_recv,
    left_send,
    right_send,
    left_recv,
    right_recv,
    halo,
    pooled,
    regrouped,
    mix,
    halo_sems,
    mix_load,
    pool_send,
    pool_recv,
    mix_send,
    mix_recv,
    pair_send,
    pair_recv,
):
    ep = lax.axis_index("ep")
    tp = lax.axis_index("tp")
    z = tp // 2
    core = tp % 2
    rows, wide = x_ref.shape
    local_experts, width, ff = gate_ref.shape
    slots = packed.shape[2]
    block = ep_size * slots
    piece = width // PIECES
    partner = (ep, tp + 1 - 2 * core)
    left = (ep, tp - 2)
    right = (ep, tp + 2)
    has_left = z > 0
    has_right = z < planes - 1
    at_end = (z * (planes - 1 - z)) == 0
    turn = 1 - 2 * (z // (planes // 2))

    inner = (z * (planes - 1 - z) + planes - 2) // (planes - 1)

    def source_of(step):
        both_ways = ((step + 1) // 2) * (2 * (step % 2) - 1)
        offset = inner * both_ways + (1 - inner) * step
        return (z + turn * offset + planes) % planes

    def sum_of(step):
        return (z + turn * step + planes) % planes

    def peer_of(offset):
        return ((ep + offset) % ep_size, tp)

    tp_size = 2 * planes
    barrier = pltpu.get_barrier_semaphore()
    for offset in range(1, ep_size):
        pl.semaphore_signal(barrier, inc=1, device_id=peer_of(offset), device_id_type=MESH)
    for offset in range(1, tp_size):
        pl.semaphore_signal(
            barrier, inc=1, device_id=(ep, (tp + offset) % tp_size), device_id_type=MESH
        )

    loads = []
    for expert in range(local_experts):
        lanes = pl.ds(expert * ff, ff)
        loads.append((gate_ref.at[expert], gate_up.at[expert, :, pl.ds(0, ff)]))
        loads.append((up_ref.at[expert], gate_up.at[expert, :, pl.ds(ff, ff)]))
        loads.append((down_ref.at[expert], down.at[:, lanes]))
    loads = [
        pltpu.make_async_copy(source, target, weight_sems.at[index])
        for index, (source, target) in enumerate(loads)
    ]
    for load in loads:
        load.start()
    mix_own = pltpu.make_async_copy(mix_ref, mix.at[tp], mix_load)
    mix_own.start()
    pl.semaphore_wait(barrier, ep_size + tp_size - 2)

    def line_copy(source_ref, source, direction):
        return pltpu.make_async_remote_copy(
            src_ref=source_ref,
            dst_ref=column.at[source],
            send_sem=line_send.at[source, direction],
            recv_sem=line_recv.at[source],
            device_id=(left, right)[direction],
            device_id_type=MESH,
        )

    def plane_copy(source, offset):
        return pltpu.make_async_remote_copy(
            src_ref=packed.at[source, offset - 1],
            dst_ref=tokens.at[source, core, pl.ds(pl.multiple_of(ep * slots, slots), slots)],
            send_sem=plane_send.at[source, offset - 1],
            recv_sem=plane_recv.at[source, offset - 1],
            device_id=peer_of(offset),
            device_id_type=MESH,
        )

    def share_copy(source):
        return pltpu.make_async_remote_copy(
            src_ref=tokens.at[source, core],
            dst_ref=tokens.at[source, core],
            send_sem=share_send.at[source],
            recv_sem=share_recv.at[source],
            device_id=partner,
            device_id_type=MESH,
        )

    def part_copy(source, slot, index):
        return pltpu.make_async_remote_copy(
            src_ref=outgoing.at[slot, index],
            dst_ref=arriving.at[slot, index],
            send_sem=part_send.at[slot, index],
            recv_sem=part_recv.at[slot, index],
            device_id=partner,
            device_id_type=MESH,
        )

    def back_copy(source, offset, index):
        target = (ep + offset) % ep_size
        return pltpu.make_async_remote_copy(
            src_ref=partial.at[source, index, pl.ds(pl.multiple_of(target * slots, slots), slots)],
            dst_ref=returned.at[source, index, pl.ds(pl.multiple_of(ep * slots, slots), slots)],
            send_sem=back_send.at[source, offset - 1, index],
            recv_sem=back_recv.at[source, offset - 1, index],
            device_id=(target, tp),
            device_id_type=MESH,
        )

    def sum_copy(source, place, index, direction):
        return pltpu.make_async_remote_copy(
            src_ref=running.at[source, index],
            dst_ref=running.at[place, index],
            send_sem=(left_send, right_send)[direction].at[source, index],
            recv_sem=(right_recv, left_recv)[direction].at[source, index],
            device_id=(left, right)[direction],
            device_id_type=MESH,
        )

    def sum_place(source, direction):
        if direction == 1:
            return source
        ends = (source + 1) // jnp.maximum(z, 1)
        return source + (planes - source) * ends

    sequence, channels = pool_ref.shape
    share_rows = sequence // tp_size
    edge = halo.shape[0]

    def halo_copy():
        return pltpu.make_async_remote_copy(
            src_ref=pool_ref.at[pl.ds(sequence - edge, edge)],
            dst_ref=halo,
            send_sem=halo_sems.at[0],
            recv_sem=halo_sems.at[1],
            device_id=peer_of(1),
            device_id_type=MESH,
        )

    def pool_copy(offset):
        target = (tp + offset) % tp_size
        lanes = pl.ds(pl.multiple_of(tp * channels, channels), channels)
        return pltpu.make_async_remote_copy(
            src_ref=pooled.at[pl.ds(pl.multiple_of(target * share_rows, share_rows), share_rows)],
            dst_ref=regrouped.at[:, lanes],
            send_sem=pool_send.at[offset - 1],
            recv_sem=pool_recv.at[offset - 1],
            device_id=(ep, target),
            device_id_type=MESH,
        )

    def mix_copy(plane, direction):
        return pltpu.make_async_remote_copy(
            src_ref=mix.at[2 * plane + core],
            dst_ref=mix.at[2 * plane + core],
            send_sem=mix_send.at[plane, direction],
            recv_sem=mix_recv.at[plane],
            device_id=(left, right)[direction],
            device_id_type=MESH,
        )

    def pair_copy(plane):
        return pltpu.make_async_remote_copy(
            src_ref=mix.at[2 * plane + core],
            dst_ref=mix.at[2 * plane + core],
            send_sem=pair_send.at[plane],
            recv_sem=pair_recv.at[plane],
            device_id=partner,
            device_id_type=MESH,
        )

    def send_mix():
        @pl.when(has_left)
        def _():
            mix_copy(z, 0).start()

        @pl.when(has_right)
        def _():
            mix_copy(z, 1).start()

        pair_copy(z).start()

    def receive_mix(plane):
        mix_copy(plane, 0).wait_recv()

        @pl.when((plane > z) & has_left)
        def _():
            mix_copy(plane, 0).start()

        @pl.when((plane < z) & has_right)
        def _():
            mix_copy(plane, 1).start()

        pair_copy(plane).start()

    def pool():
        @pl.when(ep > 0)
        def _():
            halo_copy().wait_recv()

        before = jnp.where(ep > 0, halo[...].astype(jnp.float32), 0.0)
        values = pool_ref[...].astype(jnp.float32)
        level = jnp.concatenate([before, values], axis=0)
        channel = tp * channels + lax.broadcasted_iota(jnp.int32, (1, channels), 1)
        position = ep * sequence + lax.broadcasted_iota(jnp.int32, (sequence, 1), 0)
        summed = jnp.zeros((sequence, channels), jnp.float32)
        widths = jnp.zeros((1, channels), jnp.int32)
        for index in range(4):
            level = level + pltpu.roll(level, 2**index, 0)
            inside = (channel >= index * GROUP_CH) & (channel < (index + 1) * GROUP_CH)
            summed = jnp.where(inside, level[edge:], summed)
            widths = jnp.where(inside, 2 ** (index + 1), widths)
        counted = jnp.minimum(position + 1, widths).astype(jnp.float32)
        result = (summed / counted - values) * gain_ref[...]
        pooled[...] = result.astype(jnp.bfloat16)
        own_rows = pl.ds(pl.multiple_of(tp * share_rows, share_rows), share_rows)
        lanes = pl.ds(pl.multiple_of(tp * channels, channels), channels)
        regrouped[:, lanes] = pooled[own_rows]

    def send_pooled():
        for offset in range(1, tp_size):
            pool_copy(offset).start()

    def mixer():
        for offset in range(1, tp_size):
            pool_copy(offset).wait_recv()
        for plane in range(planes):
            pair_copy(plane).wait_recv()
        total = jnp.zeros((share_rows, mix.shape[2]), jnp.float32)
        for index in range(tp_size):
            part = regrouped[:, index * channels : (index + 1) * channels]
            total = total + jnp.dot(part, mix[index], preferred_element_type=jnp.float32)
        mixed_ref[...] = total.astype(jnp.bfloat16)

    def dispatch(source_ref, source):
        routing = source_ref[:, width:].astype(jnp.float32).T
        for offset in range(ep_size):
            group = (ep + offset) % ep_size
            slot_row = jnp.zeros((1, rows), jnp.float32)
            for index in range(ep_size):
                row = 2 * local_experts + index
                chosen = jnp.where(index == group, 1.0, 0.0)
                slot_row = slot_row + routing[row : row + 1] * chosen
            places = lax.broadcasted_iota(jnp.int32, (slots, rows), 0).astype(jnp.float32)
            placing = jnp.where(places == slot_row, 1.0, 0.0).astype(jnp.bfloat16)
            compact = jnp.dot(placing, source_ref[...], preferred_element_type=jnp.float32)
            compact = compact.astype(jnp.bfloat16)
            if offset == 0:
                tokens[source, core, pl.ds(pl.multiple_of(ep * slots, slots), slots)] = compact
            else:
                packed[source, offset - 1] = compact
                plane_copy(source, offset).start()

    def gather(source):
        for offset in range(1, ep_size):
            plane_copy(source, offset).wait_recv()
        share_copy(source).start()

    def experts(source, slot):
        share_copy(source).wait_recv()

        def one(expert, carry):
            values = tokens[source].reshape(2 * block, wide)
            both = jnp.dot(
                values[:, :width], gate_up[expert], preferred_element_type=jnp.float32
            )
            lane = lax.broadcasted_iota(jnp.int32, (2 * block, LANES), 1)
            mine = (lane == expert) | (lane == local_experts + expert)
            scale = jnp.where(mine, values[:, width:].astype(jnp.float32), 0.0)
            scale = jnp.sum(scale, axis=1, keepdims=True)
            gated = both[:, :ff]
            gated = gated / (1.0 + jnp.exp(-gated))
            result = (gated * both[:, ff:] * scale).astype(jnp.bfloat16)
            hidden[:, pl.ds(pl.multiple_of(expert * ff, ff), ff)] = result
            return carry

        lax.fori_loop(0, local_experts, one, 0)

        def project(which, index):
            part = hidden[pl.ds(pl.multiple_of(which * block, block), block)]
            return lax.dot_general(
                part,
                down[index * piece : (index + 1) * piece],
                (((1,), (1,)), ((), ())),
                preferred_element_type=jnp.float32,
            )

        for index in range(PIECES):
            outgoing[slot, index] = project(1 - core, index).astype(jnp.bfloat16)
            part_copy(source, slot, index).start()
        for index in range(PIECES):
            own = project(core, index)
            part_copy(source, slot, index).wait_recv()
            total = own + arriving[slot, index].astype(jnp.float32)
            partial[source, index] = total.astype(jnp.bfloat16)
            own_rows = pl.ds(pl.multiple_of(ep * slots, slots), slots)
            returned[source, index, own_rows] = partial[source, index, own_rows]

            @pl.when(source != z)
            def _():
                for offset in range(1, ep_size):
                    back_copy(source, offset, index).start()

    def placing_back(source_ref):
        routing = source_ref[:, width:].astype(jnp.float32)
        pieces = []
        for group in range(ep_size):
            lane = 2 * local_experts + group
            places = lax.broadcasted_iota(jnp.int32, (rows, slots), 1).astype(jnp.float32)
            matched = places == routing[:, lane : lane + 1]
            pieces.append(jnp.where(matched, 1.0, 0.0))
        return jnp.concatenate(pieces, axis=1).astype(jnp.bfloat16)

    def combine(placing, source, index):
        for offset in range(1, ep_size):
            back_copy(source, offset, index).wait_recv()
        return jnp.dot(placing, returned[source, index], preferred_element_type=jnp.float32)

    def reduce_piece(source, placing, index):
        mine = combine(placing, source, index)
        for direction in range(2):
            toward = (source < z, source > z)[direction]
            has_before = (has_right, has_left)[direction]

            @pl.when(toward & has_before)
            def _(direction=direction):
                sum_copy(source, source, index, direction).wait_recv()
                total = mine + running[source, index].astype(jnp.float32)
                running[source, index] = total.astype(jnp.bfloat16)
                place = sum_place(source, direction)
                sum_copy(source, place, index, direction).start()

            @pl.when(toward & ~has_before)
            def _(direction=direction):
                running[source, index] = mine.astype(jnp.bfloat16)
                place = sum_place(source, direction)
                sum_copy(source, place, index, direction).start()

    def reduce_line(*steps):
        sources = [sum_of(step) for step in steps]
        placings = [placing_back(column.at[source]) for source in sources]
        for index in range(PIECES):
            for source, placing in zip(sources, placings):
                reduce_piece(source, placing, index)

    @pl.when(has_left)
    def _():
        line_copy(x_ref, z, 0).start()

    @pl.when(has_right)
    def _():
        line_copy(x_ref, z, 1).start()

    mix_own.wait()

    @pl.when(at_end)
    def _():
        send_mix()

    @pl.when(ep < ep_size - 1)
    def _():
        halo_copy().start()

    dispatch(x_ref, z)
    pool()
    for load in loads:
        load.wait()

    def receive(source):
        line_copy(x_ref, source, 0).wait_recv()

        @pl.when((source > z) & has_left)
        def _():
            line_copy(column.at[source], source, 0).start()

        @pl.when((source < z) & has_right)
        def _():
            line_copy(column.at[source], source, 1).start()

    def step_body(step, carry):
        current = source_of(step)

        @pl.when((at_end & (step < planes)) | (~at_end & (step == 1)))
        def _():
            receive(current)

        @pl.when(step < planes)
        def _():
            dispatch(column.at[current], current)

        @pl.when(~at_end & (step == 1))
        def _():
            receive(source_of(2))

        @pl.when(at_end & (step == 2))
        def _():
            send_pooled()

        previous = source_of(step - 1)
        slot = (step - 1) % 2
        gather(previous)

        @pl.when(~at_end & (step == 2))
        def _():
            receive(source_of(3))

        @pl.when(~at_end & (step == planes))
        def _():
            send_mix()
            send_pooled()
            receive_mix(source_of(2))

        @pl.when(at_end & (step == planes - 1))
        def _():
            reduce_line(1)

        @pl.when(step > 2)
        def _():
            for index in range(PIECES):
                part_copy(previous, slot, index).wait_send()

        experts(previous, slot)

        return carry

    lax.fori_loop(1, planes + 1, step_body, 0)
    for index in range(PIECES):
        for offset in range(1, ep_size):
            back_copy(z, offset, index).start()

    @pl.when(at_end)
    def _():
        for step in range(2, planes):
            reduce_line(step)

        for step in range(1, planes):
            receive_mix(sum_of(step))

    @pl.when(~at_end)
    def _():
        receive_mix(source_of(1))
        receive_mix(source_of(3))
        reduce_line(1)
        reduce_line(2, 3)

    mixer()
    placing = placing_back(x_ref)
    for index in range(PIECES):
        mine = combine(placing, z, index)
        lanes = pl.ds(index * piece, piece)

        for direction in range(2):
            has_before = (has_right, has_left)[direction]

            @pl.when(has_before)
            def _(direction=direction):
                sum_copy(z, z, index, direction).wait_recv()

        zero = jnp.zeros_like(mine)
        from_left = jnp.where(has_left, running[z, index].astype(jnp.float32), zero)
        from_right = jnp.where(has_right, running[planes, index].astype(jnp.float32), zero)
        out_ref[:, lanes] = (mine + from_left + from_right).astype(jnp.bfloat16)

    @pl.when(has_left)
    def _():
        line_copy(x_ref, z, 0).wait_send()

    @pl.when(has_right)
    def _():
        line_copy(x_ref, z, 1).wait_send()

    @pl.when(ep < ep_size - 1)
    def _():
        halo_copy().wait_send()

    for offset in range(1, tp_size):
        pool_copy(offset).wait_send()
    for direction in range(2):

        @pl.when((has_left, has_right)[direction])
        def _(direction=direction):
            mix_copy(z, direction).wait_send()


    def drain(source, carry):
        for offset in range(1, ep_size):
            plane_copy(source, offset).wait_send()
            for index in range(PIECES):
                back_copy(source, offset, index).wait_send()
        share_copy(source).wait_send()
        pair_copy(source).wait_send()
        for direction in range(2):
            toward = (source < z, source > z)[direction]
            has_next = (has_left, has_right)[direction]
            forwarded = (source > z, source < z)[direction]

            @pl.when(toward)
            def _(direction=direction):
                for index in range(PIECES):
                    sum_copy(source, source, index, direction).wait_send()

            @pl.when(forwarded & has_next)
            def _(direction=direction):
                line_copy(x_ref, source, direction).wait_send()
                mix_copy(source, direction).wait_send()

        return carry

    lax.fori_loop(0, planes, drain, 0)
    for slot in range(2):
        for index in range(PIECES):
            part_copy(0, slot, index).wait_send()


def fused_layers(extended, pool_input, pool_gain, mix_weight, weights, ep_size, planes, slots):
    gate_weight, up_weight, down_weight = weights
    rows, wide = extended.shape
    sequence, channels = pool_input.shape
    depth, outputs = mix_weight.shape
    tp_size = 2 * planes
    share_rows = sequence // tp_size
    edge = 16
    local_experts, width, ff = gate_weight.shape
    block = ep_size * slots
    piece = width // PIECES
    half = jnp.bfloat16
    dma = pltpu.SemaphoreType.DMA
    return pl.pallas_call(
        functools.partial(expert_kernel, ep_size, planes),
        out_shape=(
            jax.ShapeDtypeStruct((share_rows, outputs), half),
            jax.ShapeDtypeStruct((rows, width), half),
        ),
        in_specs=[pl.BlockSpec(memory_space=pltpu.VMEM)] * 3
        + [pl.BlockSpec(memory_space=pl.ANY)] * 4,
        out_specs=(pl.BlockSpec(memory_space=pltpu.VMEM),) * 2,
        scratch_shapes=[
            pltpu.VMEM((planes, rows, wide), half),
            pltpu.VMEM((planes, ep_size - 1, slots, wide), half),
            pltpu.VMEM((planes, 2, block, wide), half),
            pltpu.VMEM((local_experts, width, 2 * ff), half),
            pltpu.VMEM((width, local_experts * ff), half),
            pltpu.VMEM((2 * block, local_experts * ff), half),
            pltpu.VMEM((2, PIECES, block, piece), half),
            pltpu.VMEM((planes, PIECES, block, piece), half),
            pltpu.VMEM((2, PIECES, block, piece), half),
            pltpu.VMEM((planes, PIECES, block, piece), half),
            pltpu.VMEM((planes + 1, PIECES, rows, piece), half),
            dma((3 * local_experts,)),
            dma((planes, 2)),
            dma((planes,)),
            dma((planes, ep_size - 1)),
            dma((planes, ep_size - 1)),
            dma((planes,)),
            dma((planes,)),
            dma((2, PIECES)),
            dma((2, PIECES)),
            dma((planes, ep_size - 1, PIECES)),
            dma((planes, ep_size - 1, PIECES)),
            dma((planes, PIECES)),
            dma((planes, PIECES)),
            dma((planes, PIECES)),
            dma((planes, PIECES)),
            pltpu.VMEM((edge, channels), half),
            pltpu.VMEM((sequence, channels), half),
            pltpu.VMEM((share_rows, tp_size * channels), half),
            pltpu.VMEM((tp_size, depth, outputs), half),
            dma((2,)),
            dma,
            dma((tp_size - 1,)),
            dma((tp_size - 1,)),
            dma((planes, 2)),
            dma((planes,)),
            dma((planes,)),
            dma((planes,)),
        ],
        compiler_params=pltpu.CompilerParams(
            collective_id=0, has_side_effects=True, vmem_limit_bytes=VMEM_LIMIT
        ),
    )(extended, pool_input, pool_gain[None, :], mix_weight, gate_weight, up_weight, down_weight)


def routing_lanes(expert_ids, route_weight, ep_size):
    local_experts = EXPERTS // ep_size
    owners = expert_ids // local_experts
    ep_index = lax.iota(jnp.int32, ep_size)
    member = jnp.any(owners[:, :, None] == ep_index[None, None, :], axis=1)
    counts = member.astype(jnp.int32)
    rank = jnp.cumsum(counts, axis=0) - counts
    slot = jnp.where(member, rank, -1).astype(jnp.float32)
    within = expert_ids % local_experts
    named = within[:, :, None] == lax.iota(jnp.int32, local_experts)[None, None, :]
    weights = jnp.sum(jnp.where(named, route_weight[:, :, None], 0.0), axis=1)
    high = lax.reduce_precision(weights, 8, 7)
    low = weights - high
    spare = LANES - 2 * local_experts - ep_size
    lanes = jnp.concatenate([high, low, slot], axis=1)
    return jnp.pad(lanes, ((0, 0), (0, spare))).astype(jnp.bfloat16)


def fast_body(
    pool_input,
    pool_gain,
    mix_weight,
    moe_input,
    moe_gain,
    expert_ids,
    route_weight,
    gate_weight,
    up_weight,
    down_weight,
):
    ep_size = lax.axis_size("ep")
    planes = lax.axis_size("tp") // 2
    local_experts = gate_weight.shape[0]
    slots = local_experts * CAP // TOP
    inputs = moe_input.astype(jnp.float32)
    scale_rows = lax.rsqrt(jnp.mean(inputs * inputs, axis=-1, keepdims=True) + eps_norm)
    normed = (inputs * scale_rows * moe_gain).astype(jnp.bfloat16)
    extended = jnp.concatenate([normed, routing_lanes(expert_ids, route_weight, ep_size)], axis=1)
    return fused_layers(
        extended,
        pool_input,
        pool_gain,
        mix_weight,
        (gate_weight, up_weight, down_weight),
        ep_size,
        planes,
        slots,
    )


def fits(mesh, shapes):
    pool_input, mix_weight, moe_input, gate_weight = shapes
    ep_size = mesh.shape["ep"]
    tp_size = mesh.shape["tp"]
    experts, width, ff = gate_weight
    local_experts = experts // ep_size
    rows = moe_input[0] // (ep_size * tp_size)
    ff = ff // tp_size
    if local_experts % GROUP_EXP or tp_size % 4 or tp_size > 8 or ff % LANES or width % (PIECES * LANES):
        return False
    if 2 * local_experts + ep_size > LANES or rows > 256:
        return False
    slots = local_experts * CAP // TOP
    if slots % 16 or rows % 16:
        return False
    sequence = pool_input[0] // ep_size
    channels = pool_input[1] // tp_size
    share_rows = sequence // tp_size
    if channels % LANES or mix_weight[0] != pool_input[1] or share_rows % 16 or mix_weight[1] % LANES:
        return False
    mixer = mix_weight[0] * mix_weight[1] + share_rows * (mix_weight[0] + mix_weight[1])
    mixer += 2 * sequence * channels
    needed = kernel_bytes(ep_size, tp_size // 2, rows, slots, width, ff, local_experts, mixer)
    return needed < VMEM_LIMIT


def solution(mesh):
    def program(*arguments):
        shapes = tuple(arguments[index].shape for index in (0, 2, 3, 7))
        body = fast_body if fits(mesh, shapes) else general_body
        return jax.shard_map(
            body,
            mesh=mesh,
            in_specs=(
                P("ep", "tp"),
                P("tp"),
                P("tp", None),
                P(("ep", "tp"), None),
                P(),
                P(("ep", "tp"), None),
                P(("ep", "tp"), None),
                P("ep", None, "tp"),
                P("ep", None, "tp"),
                P("ep", None, "tp"),
            ),
            out_specs=(P(("ep", "tp"), None), P(("ep", "tp"), None)),
            check_vma=False,
        )(*arguments)

    return program
```

```python
import functools

import jax
import jax.numpy as jnp
from jax import lax
from jax.experimental import pallas as pl
from jax.experimental.pallas import tpu as pltpu
from jax.sharding import PartitionSpec as P

GROUP_CH = 256
EXPERTS = 16
GROUP_EXP = 4
TOP = 2
CAP = 48
CHUNKS = 2


eps_norm = 1e-06


def from_behind(shard, axis, by):
    peers = lax.axis_size(axis)
    pairs = [(i, i + by) for i in range(peers) if 0 <= i + by < peers]
    return lax.ppermute(shard, axis, pairs)


def window_sums(extended, row_count):
    level_sum = extended
    stride = 1
    outputs = []
    for doubling in range(4):
        level_sum = level_sum[stride:] + level_sum[:-stride]
        stride = stride * 2
        outputs.append(level_sum[level_sum.shape[0] - row_count :])
    return outputs


def pool_mixer(pool_input, pool_gain):
    row_count, channels = pool_input.shape
    carried = from_behind(pool_input[row_count - 15 :], "ep", 1)
    extended = jnp.concatenate([carried, pool_input], axis=0).astype(jnp.float32)
    window_list = window_sums(extended, row_count)
    channel_ids = lax.axis_index("tp") * channels + lax.iota(jnp.int32, channels)
    group_ids = channel_ids // GROUP_CH
    position = lax.axis_index("ep") * row_count + lax.iota(jnp.int32, row_count)
    summed = jnp.zeros((row_count, channels), jnp.float32)
    widths = jnp.zeros((channels,), jnp.int32)
    for index_group in range(4):
        inside = group_ids == index_group
        summed = jnp.where(inside[None, :], window_list[index_group], summed)
        widths = jnp.where(inside, 2 ** (index_group + 1), widths)
    counted = jnp.minimum(position[:, None] + 1, widths[None, :]).astype(jnp.float32)
    values = extended[15:]
    return ((summed / counted - values) * pool_gain).astype(jnp.bfloat16)


def dispatch_plan(expert_ids, route_weight, ep_size):
    local_experts = EXPERTS // ep_size
    share = TOP if local_experts % GROUP_EXP == 0 else 1
    capacity = local_experts * CAP // share
    owners = expert_ids // local_experts
    ep_index = lax.iota(jnp.int32, ep_size)
    member = jnp.any(owners[:, :, None] == ep_index[None, None, :], axis=1)
    counts = member.astype(jnp.int32)
    rank = jnp.cumsum(counts, axis=0) - counts
    slot = jnp.where(member, rank, -1).T
    placing = slot[:, None, :] == lax.iota(jnp.int32, capacity)[None, :, None]
    dense_weight = jnp.sum(
        jnp.where(
            expert_ids[:, :, None] == lax.iota(jnp.int32, EXPERTS)[None, None, :],
            route_weight[:, :, None],
            0.0,
        ),
        axis=1,
    )
    dense_weight = dense_weight.reshape(-1, ep_size, local_experts)
    slot_weight = jnp.einsum(
        "ecn,nej->ecj",
        placing.astype(jnp.float32),
        dense_weight,
        precision=lax.Precision.HIGHEST,
    )
    return placing.astype(jnp.bfloat16).reshape(ep_size * capacity, -1), slot_weight, capacity


def general_body(
    pool_input,
    pool_gain,
    mix_weight,
    moe_input,
    moe_gain,
    expert_ids,
    route_weight,
    gate_weight,
    up_weight,
    down_weight,
):
    pooled = pool_mixer(pool_input, pool_gain)
    ep_size = lax.axis_size("ep")
    out_columns = mix_weight.shape[1] // ep_size
    mix_columns = lax.dynamic_slice_in_dim(
        mix_weight, lax.axis_index("ep") * out_columns, out_columns, axis=1
    )
    mix_columns = lax.all_gather(mix_columns, "tp", axis=0, tiled=True)
    inputs = moe_input.astype(jnp.float32)
    scale_rows = lax.rsqrt(jnp.mean(inputs * inputs, axis=-1, keepdims=True) + eps_norm)
    normed = (inputs * scale_rows * moe_gain).astype(jnp.bfloat16)
    placing, slot_weight, capacity = dispatch_plan(expert_ids, route_weight, ep_size)
    rows = capacity // CHUNKS
    arrived_list = []
    placing_list = []
    for chunk in range(CHUNKS):
        chunk_placing = placing.reshape(ep_size, capacity, -1)[:, chunk * rows : (chunk + 1) * rows]
        chunk_placing = chunk_placing.reshape(ep_size * rows, -1)
        outgoing = jnp.dot(chunk_placing, normed, preferred_element_type=jnp.float32)
        outgoing = outgoing.astype(jnp.bfloat16)
        placing_list.append(chunk_placing)
        arrived_list.append(
            lax.all_to_all(outgoing, "ep", split_axis=0, concat_axis=0, tiled=True)
        )
    arrived_list[0], mix_columns = lax.optimization_barrier((arrived_list[0], mix_columns))
    weights = lax.all_to_all(slot_weight, "ep", split_axis=0, concat_axis=0, tiled=True)
    weights = lax.all_gather(weights, "tp", axis=0, tiled=True)
    combined = jnp.zeros(normed.shape, jnp.float32)
    for chunk in range(CHUNKS):
        tokens = lax.all_gather(arrived_list[chunk], "tp", axis=0, tiled=True)
        scales = weights[:, chunk * rows : (chunk + 1) * rows].reshape(tokens.shape[0], -1)
        gate_part = jnp.einsum(
            "nd,edf->enf", tokens, gate_weight, preferred_element_type=jnp.float32
        )
        upward = jnp.einsum("nd,edf->enf", tokens, up_weight, preferred_element_type=jnp.float32)
        hidden = (jax.nn.silu(gate_part) * upward * scales.T[:, :, None]).astype(jnp.bfloat16)
        partial = jnp.einsum("enf,edf->nd", hidden, down_weight, preferred_element_type=jnp.float32)
        reduced = lax.psum_scatter(
            partial.astype(jnp.bfloat16), "tp", scatter_dimension=0, tiled=True
        )
        returned = lax.all_to_all(reduced, "ep", split_axis=0, concat_axis=0, tiled=True)
        combined = combined + lax.dot_general(
            placing_list[chunk],
            returned,
            (((0,), (0,)), ((), ())),
            preferred_element_type=jnp.float32,
        )
    moe_out = combined.astype(jnp.bfloat16)
    regrouped = lax.all_to_all(pooled, "tp", split_axis=0, concat_axis=1, tiled=True)
    half = regrouped.shape[1] // 2
    mixed_sum = 0.0
    for part in range(2):
        section = slice(part * half, (part + 1) * half)
        pooled_rows = lax.all_gather(regrouped[:, section], "ep", axis=0, tiled=True)
        mixed_sum = mixed_sum + jnp.dot(
            pooled_rows, mix_columns[section], preferred_element_type=jnp.float32
        )
    mixed_out = lax.all_to_all(
        mixed_sum.astype(jnp.bfloat16), "ep", split_axis=0, concat_axis=1, tiled=True
    )
    return (mixed_out, moe_out)


LANES = 128
PIECES = 4
VMEM_LIMIT = 67043328
MESH = pl.DeviceIdType.MESH


def kernel_bytes(ep_size, planes, rows, slots, width, hidden, local_experts, mixer_elements):
    wide = width + LANES
    block = ep_size * slots
    elements = planes * rows * wide
    elements += planes * (ep_size - 1) * slots * wide
    elements += planes * 2 * block * wide
    elements += 3 * local_experts * width * hidden
    elements += (planes * 2 + 4) * block * width
    elements += (planes + 1) * rows * width
    elements += 2 * block * local_experts * hidden
    elements += rows * (wide + width)
    elements += mixer_elements
    return 2 * elements


def expert_kernel(
    ep_size,
    planes,
    x_ref,
    pool_ref,
    gain_ref,
    mix_ref,
    gate_ref,
    up_ref,
    down_ref,
    mixed_ref,
    out_ref,
    column,
    packed,
    tokens,
    gate_up,
    down,
    hidden,
    outgoing,
    partial,
    arriving,
    returned,
    running,
    weight_sems,
    line_send,
    line_recv,
    plane_send,
    plane_recv,
    share_send,
    share_recv,
    part_send,
    part_recv,
    back_send,
    back_recv,
    left_send,
    right_send,
    left_recv,
    right_recv,
    halo,
    pooled,
    regrouped,
    mix,
    halo_sems,
    mix_load,
    pool_send,
    pool_recv,
    block_send,
    block_recv,
    total_send,
    total_recv,
    mix_send,
    mix_recv,
    pair_send,
    pair_recv,
):
    ep = lax.axis_index("ep")
    tp = lax.axis_index("tp")
    z = tp // 2
    core = tp % 2
    rows, wide = x_ref.shape
    local_experts, width, ff = gate_ref.shape
    slots = packed.shape[2]
    block = ep_size * slots
    piece = width // PIECES
    partner = (ep, tp + 1 - 2 * core)
    left = (ep, tp - 2)
    right = (ep, tp + 2)
    has_left = z > 0
    has_right = z < planes - 1
    at_end = (z * (planes - 1 - z)) == 0
    turn = 1 - 2 * (z // (planes // 2))

    inner = (z * (planes - 1 - z) + planes - 2) // (planes - 1)

    def source_of(step):
        both_ways = ((step + 1) // 2) * (2 * (step % 2) - 1)
        far_first = step + (step // 2) * (1 - 2 * (step % 2))
        offset = inner * both_ways + (1 - inner) * far_first
        return (z + turn * offset + planes) % planes

    def is_end(source):
        return (source * (planes - 1 - source)) == 0

    def outward(source):
        return 1 - 2 * (source // (planes // 2))

    def peer_of(offset):
        return ((ep + offset) % ep_size, tp)

    tp_size = 2 * planes
    barrier = pltpu.get_barrier_semaphore()
    for offset in range(1, ep_size):
        pl.semaphore_signal(barrier, inc=1, device_id=peer_of(offset), device_id_type=MESH)
    for offset in range(1, tp_size):
        pl.semaphore_signal(
            barrier, inc=1, device_id=(ep, (tp + offset) % tp_size), device_id_type=MESH
        )

    loads = []
    for expert in range(local_experts):
        lanes = pl.ds(expert * ff, ff)
        loads.append((gate_ref.at[expert], gate_up.at[expert, :, pl.ds(0, ff)]))
        loads.append((up_ref.at[expert], gate_up.at[expert, :, pl.ds(ff, ff)]))
        loads.append((down_ref.at[expert], down.at[:, lanes]))
    loads = [
        pltpu.make_async_copy(source, target, weight_sems.at[index])
        for index, (source, target) in enumerate(loads)
    ]
    for load in loads:
        load.start()
    mix_own = pltpu.make_async_copy(mix_ref, mix.at[tp], mix_load)
    mix_own.start()
    pl.semaphore_wait(barrier, ep_size + tp_size - 2)

    def line_copy(source_ref, source, direction):
        return pltpu.make_async_remote_copy(
            src_ref=source_ref,
            dst_ref=column.at[source],
            send_sem=line_send.at[source, direction],
            recv_sem=line_recv.at[source],
            device_id=(left, right)[direction],
            device_id_type=MESH,
        )

    def plane_copy(source, offset):
        return pltpu.make_async_remote_copy(
            src_ref=packed.at[source, offset - 1],
            dst_ref=tokens.at[source, core, pl.ds(pl.multiple_of(ep * slots, slots), slots)],
            send_sem=plane_send.at[source, offset - 1],
            recv_sem=plane_recv.at[source, offset - 1],
            device_id=peer_of(offset),
            device_id_type=MESH,
        )

    def share_copy(source):
        return pltpu.make_async_remote_copy(
            src_ref=tokens.at[source, core],
            dst_ref=tokens.at[source, core],
            send_sem=share_send.at[source],
            recv_sem=share_recv.at[source],
            device_id=partner,
            device_id_type=MESH,
        )

    def part_copy(source, slot, index):
        return pltpu.make_async_remote_copy(
            src_ref=outgoing.at[slot, index],
            dst_ref=arriving.at[slot, index],
            send_sem=part_send.at[slot, index],
            recv_sem=part_recv.at[slot, index],
            device_id=partner,
            device_id_type=MESH,
        )

    def back_copy(source, offset, index):
        target = (ep + offset) % ep_size
        return pltpu.make_async_remote_copy(
            src_ref=partial.at[source, index, pl.ds(pl.multiple_of(target * slots, slots), slots)],
            dst_ref=returned.at[source, index, pl.ds(pl.multiple_of(ep * slots, slots), slots)],
            send_sem=back_send.at[source, offset - 1, index],
            recv_sem=back_recv.at[source, offset - 1, index],
            device_id=(target, tp),
            device_id_type=MESH,
        )

    def sum_copy(source, place, index, direction):
        return pltpu.make_async_remote_copy(
            src_ref=running.at[source, index],
            dst_ref=running.at[place, index],
            send_sem=(left_send, right_send)[direction].at[source, index],
            recv_sem=(right_recv, left_recv)[direction].at[source, index],
            device_id=(left, right)[direction],
            device_id_type=MESH,
        )

    def sum_place(source, direction):
        if direction == 1:
            return source
        ends = (source + 1) // jnp.maximum(z, 1)
        return source + (planes - source) * ends

    def block_copy(source, offset):
        start = pl.multiple_of(((ep - offset + ep_size) % ep_size) * slots, slots)
        return pltpu.make_async_remote_copy(
            src_ref=tokens.at[source, core, pl.ds(start, slots)],
            dst_ref=tokens.at[source, core, pl.ds(start, slots)],
            send_sem=block_send.at[source, offset],
            recv_sem=block_recv.at[source, offset],
            device_id=(ep, tp + 2 * outward(source)),
            device_id_type=MESH,
        )

    def half_rows(half):
        return pl.ds(half * (block // 2), block // 2)

    def total_copy(source, index, half):
        hops = (z - source) * outward(source)
        place = source + (planes - 1 - 2 * source) * ((planes - hops) // (planes - 1))
        return pltpu.make_async_remote_copy(
            src_ref=partial.at[source, index, half_rows(half)],
            dst_ref=returned.at[place, index, half_rows(half)],
            send_sem=total_send.at[source, 2 * index + half],
            recv_sem=total_recv.at[source, 2 * index + half],
            device_id=(ep, tp - 2 * outward(source)),
            device_id_type=MESH,
        )

    def receive_block(source, offset):
        block_copy(source, offset).wait_recv()

        @pl.when(~at_end)
        def _():
            block_copy(source, offset).start()

    sequence, channels = pool_ref.shape
    share_rows = sequence // tp_size
    edge = halo.shape[0]

    def halo_copy():
        return pltpu.make_async_remote_copy(
            src_ref=pool_ref.at[pl.ds(sequence - edge, edge)],
            dst_ref=halo,
            send_sem=halo_sems.at[0],
            recv_sem=halo_sems.at[1],
            device_id=peer_of(1),
            device_id_type=MESH,
        )

    def pool_copy(offset):
        target = (tp + offset) % tp_size
        lanes = pl.ds(pl.multiple_of(tp * channels, channels), channels)
        return pltpu.make_async_remote_copy(
            src_ref=pooled.at[pl.ds(pl.multiple_of(target * share_rows, share_rows), share_rows)],
            dst_ref=regrouped.at[:, lanes],
            send_sem=pool_send.at[offset - 1],
            recv_sem=pool_recv.at[offset - 1],
            device_id=(ep, target),
            device_id_type=MESH,
        )

    def mix_copy(plane, direction):
        return pltpu.make_async_remote_copy(
            src_ref=mix.at[2 * plane + core],
            dst_ref=mix.at[2 * plane + core],
            send_sem=mix_send.at[plane, direction],
            recv_sem=mix_recv.at[plane],
            device_id=(left, right)[direction],
            device_id_type=MESH,
        )

    def pair_copy(plane):
        return pltpu.make_async_remote_copy(
            src_ref=mix.at[2 * plane + core],
            dst_ref=mix.at[2 * plane + core],
            send_sem=pair_send.at[plane],
            recv_sem=pair_recv.at[plane],
            device_id=partner,
            device_id_type=MESH,
        )

    def send_mix():
        @pl.when(has_left)
        def _():
            mix_copy(z, 0).start()

        @pl.when(has_right)
        def _():
            mix_copy(z, 1).start()

        pair_copy(z).start()

    def receive_mix(plane):
        mix_copy(plane, 0).wait_recv()

        @pl.when((plane > z) & has_left)
        def _():
            mix_copy(plane, 0).start()

        @pl.when((plane < z) & has_right)
        def _():
            mix_copy(plane, 1).start()

        pair_copy(plane).start()

    def pool():
        @pl.when(ep > 0)
        def _():
            halo_copy().wait_recv()

        before = jnp.where(ep > 0, halo[...].astype(jnp.float32), 0.0)
        values = pool_ref[...].astype(jnp.float32)
        level = jnp.concatenate([before, values], axis=0)
        channel = tp * channels + lax.broadcasted_iota(jnp.int32, (1, channels), 1)
        position = ep * sequence + lax.broadcasted_iota(jnp.int32, (sequence, 1), 0)
        summed = jnp.zeros((sequence, channels), jnp.float32)
        widths = jnp.zeros((1, channels), jnp.int32)
        for index in range(4):
            level = level + pltpu.roll(level, 2**index, 0)
            inside = (channel >= index * GROUP_CH) & (channel < (index + 1) * GROUP_CH)
            summed = jnp.where(inside, level[edge:], summed)
            widths = jnp.where(inside, 2 ** (index + 1), widths)
        counted = jnp.minimum(position + 1, widths).astype(jnp.float32)
        result = (summed / counted - values) * gain_ref[...]
        pooled[...] = result.astype(jnp.bfloat16)
        own_rows = pl.ds(pl.multiple_of(tp * share_rows, share_rows), share_rows)
        lanes = pl.ds(pl.multiple_of(tp * channels, channels), channels)
        regrouped[:, lanes] = pooled[own_rows]

    def send_pooled():
        for offset in range(1, tp_size):
            pool_copy(offset).start()

    def mixer():
        for offset in range(1, tp_size):
            pool_copy(offset).wait_recv()
        for plane in range(planes):
            pair_copy(plane).wait_recv()
        total = jnp.zeros((share_rows, mix.shape[2]), jnp.float32)
        for index in range(tp_size):
            part = regrouped[:, index * channels : (index + 1) * channels]
            total = total + jnp.dot(part, mix[index], preferred_element_type=jnp.float32)
        mixed_ref[...] = total.astype(jnp.bfloat16)

    def dispatch(source_ref, source):
        routing = source_ref[:, width:].astype(jnp.float32).T
        for offset in range(ep_size):
            group = (ep + offset) % ep_size
            slot_row = jnp.zeros((1, rows), jnp.float32)
            for index in range(ep_size):
                row = 2 * local_experts + index
                chosen = jnp.where(index == group, 1.0, 0.0)
                slot_row = slot_row + routing[row : row + 1] * chosen
            places = lax.broadcasted_iota(jnp.int32, (slots, rows), 0).astype(jnp.float32)
            placing = jnp.where(places == slot_row, 1.0, 0.0).astype(jnp.bfloat16)
            compact = jnp.dot(placing, source_ref[...], preferred_element_type=jnp.float32)
            compact = compact.astype(jnp.bfloat16)
            if offset == 0:
                tokens[source, core, pl.ds(pl.multiple_of(ep * slots, slots), slots)] = compact
            else:
                packed[source, offset - 1] = compact
                plane_copy(source, offset).start()

    def gather(source):
        for offset in range(1, ep_size):
            plane_copy(source, offset).wait_recv()
        share_copy(source).start()

    def keep_own(source, index):
        own_rows = pl.ds(pl.multiple_of(ep * slots, slots), slots)
        returned[source, index, own_rows] = partial[source, index, own_rows]

    def experts(source, slot):
        share_copy(source).wait_recv()

        def one(expert, carry):
            values = tokens[source].reshape(2 * block, wide)
            both = jnp.dot(
                values[:, :width], gate_up[expert], preferred_element_type=jnp.float32
            )
            lane = lax.broadcasted_iota(jnp.int32, (2 * block, LANES), 1)
            mine = (lane == expert) | (lane == local_experts + expert)
            scale = jnp.where(mine, values[:, width:].astype(jnp.float32), 0.0)
            scale = jnp.sum(scale, axis=1, keepdims=True)
            gated = both[:, :ff]
            gated = gated / (1.0 + jnp.exp(-gated))
            result = (gated * both[:, ff:] * scale).astype(jnp.bfloat16)
            hidden[:, pl.ds(pl.multiple_of(expert * ff, ff), ff)] = result
            return carry

        lax.fori_loop(0, local_experts, one, 0)

        def project(which, index):
            part = hidden[pl.ds(pl.multiple_of(which * block, block), block)]
            return lax.dot_general(
                part,
                down[index * piece : (index + 1) * piece],
                (((1,), (1,)), ((), ())),
                preferred_element_type=jnp.float32,
            )

        for index in range(PIECES):
            outgoing[slot, index] = project(1 - core, index).astype(jnp.bfloat16)
            part_copy(source, slot, index).start()
        for index in range(PIECES):
            own = project(core, index)
            part_copy(source, slot, index).wait_recv()
            total = own + arriving[slot, index].astype(jnp.float32)
            partial[source, index] = total.astype(jnp.bfloat16)

            @pl.when(~is_end(source))
            def _():
                keep_own(source, index)

            @pl.when(~is_end(source))
            def _():
                for offset in range(1, ep_size):
                    back_copy(source, offset, index).start()

            @pl.when(is_end(source) & at_end & (source != z))
            def _():
                for half in range(2):
                    total_copy(source, index, half).start()

    def placing_back(source_ref):
        routing = source_ref[:, width:].astype(jnp.float32)
        pieces = []
        for group in range(ep_size):
            lane = 2 * local_experts + group
            places = lax.broadcasted_iota(jnp.int32, (rows, slots), 1).astype(jnp.float32)
            matched = places == routing[:, lane : lane + 1]
            pieces.append(jnp.where(matched, 1.0, 0.0))
        return jnp.concatenate(pieces, axis=1).astype(jnp.bfloat16)

    def combine(placing, source, index):
        for offset in range(1, ep_size):
            back_copy(source, offset, index).wait_recv()
        return jnp.dot(placing, returned[source, index], preferred_element_type=jnp.float32)

    def reduce_piece(source, placing, index):
        mine = combine(placing, source, index)
        for direction in range(2):
            toward = (source < z, source > z)[direction]
            has_before = (has_right, has_left)[direction]

            @pl.when(toward & has_before)
            def _(direction=direction):
                sum_copy(source, source, index, direction).wait_recv()
                total = mine + running[source, index].astype(jnp.float32)
                running[source, index] = total.astype(jnp.bfloat16)
                place = sum_place(source, direction)
                sum_copy(source, place, index, direction).start()

            @pl.when(toward & ~has_before)
            def _(direction=direction):
                running[source, index] = mine.astype(jnp.bfloat16)
                place = sum_place(source, direction)
                sum_copy(source, place, index, direction).start()

    def reduce_line(source):
        placing = placing_back(column.at[source])
        for index in range(PIECES):
            reduce_piece(source, placing, index)

    def add_total(source, place, index, half):
        total_copy(source, index, half).wait_recv()
        which = half_rows(half)
        total = partial[source, index, which].astype(jnp.float32)
        total = total + returned[place, index, which].astype(jnp.float32)
        partial[source, index, which] = total.astype(jnp.bfloat16)

    def pass_total(source, index, half):
        add_total(source, source, index, half)
        total_copy(source, index, half).start()

    def receive(source):
        line_copy(x_ref, source, 0).wait_recv()

        @pl.when((source > z) & has_left)
        def _():
            line_copy(column.at[source], source, 0).start()

        @pl.when((source < z) & has_right)
        def _():
            line_copy(column.at[source], source, 1).start()

    @pl.when(~at_end)
    def _():
        line_copy(x_ref, z, 0).start()
        line_copy(x_ref, z, 1).start()

    @pl.when(ep < ep_size - 1)
    def _():
        halo_copy().start()

    dispatch(x_ref, z)

    @pl.when(at_end)
    def _():
        block_copy(z, 0).start()

    pool()

    @pl.when(at_end)
    def _():
        for offset in range(1, ep_size):
            plane_copy(z, offset).wait_recv()
            block_copy(z, offset).start()
        share_copy(z).start()

    mix_own.wait()
    for load in loads:
        load.wait()

    def step_body(step, carry):
        current = source_of(step)
        slot = step % 2

        @pl.when(step == 0)
        def _():
            receive(source_of(1))
            dispatch(column.at[source_of(1)], source_of(1))

        @pl.when(at_end & (step == 1))
        def _():
            send_mix()
            send_pooled()

        @pl.when(at_end & (step == 2))
        def _():
            reduce_line(source_of(1))

        @pl.when(~at_end & (step == 0))
        def _():
            receive_block(source_of(2), 0)
            receive_block(source_of(2), 1)

        @pl.when(~at_end & (step == 1))
        def _():
            receive_block(source_of(2), 2)
            receive_block(source_of(2), 3)
            receive_block(source_of(3), 0)

        @pl.when(~is_end(current))
        def _():
            gather(current)

        @pl.when(~at_end & (step == 1))
        def _():
            receive_block(source_of(3), 1)

        @pl.when(~at_end & (step == 2))
        def _():
            receive_block(source_of(3), 2)

        @pl.when(~at_end & (step == 3))
        def _():
            receive_block(source_of(3), 3)
            send_mix()
            send_pooled()
            receive_mix(source_of(2))

        @pl.when(at_end & (step == 2))
        def _():
            for offset in range(ep_size):
                receive_block(current, offset)

        @pl.when(is_end(current) & (current != z))
        def _():
            share_copy(current).start()

        @pl.when(step > 1)
        def _():
            for index in range(PIECES):
                part_copy(current, slot, index).wait_send()

        experts(current, slot)

        @pl.when(at_end & (step == 1))
        def _():
            receive(source_of(3))
            dispatch(column.at[source_of(3)], source_of(3))

        return carry

    lax.fori_loop(0, planes, step_body, 0)

    @pl.when(at_end)
    def _():
        for index in range(PIECES - 1):
            for half in range(2):
                total_copy(source_of(2), index, half).wait_send()
        reduce_line(source_of(3))
        for step in range(1, planes):
            receive_mix(source_of(step))
        for index in range(PIECES):
            for half in range(2):
                add_total(z, planes - 1 - z, index, half)
            keep_own(z, index)
            for offset in range(1, ep_size):
                back_copy(z, offset, index).start()

    @pl.when(~at_end)
    def _():
        receive_mix(source_of(1))
        receive_mix(source_of(3))
        for index in range(PIECES):
            for half in range(2):
                pass_total(source_of(3), index, half)
                pass_total(source_of(2), index, half)
        reduce_line(source_of(1))

    mixer()

    placing = placing_back(x_ref)
    for index in range(PIECES):
        mine = combine(placing, z, index)
        lanes = pl.ds(index * piece, piece)

        @pl.when(~at_end)
        def _():
            sum_copy(z, z, index, 0).wait_recv()
            sum_copy(z, z, index, 1).wait_recv()
            others = running[z, index].astype(jnp.float32)
            others = others + running[planes, index].astype(jnp.float32)
            out_ref[:, lanes] = (mine + others).astype(jnp.bfloat16)

        @pl.when(at_end)
        def _():
            out_ref[:, lanes] = mine.astype(jnp.bfloat16)

    @pl.when(~at_end)
    def _():
        line_copy(x_ref, z, 0).wait_send()
        line_copy(x_ref, z, 1).wait_send()

    @pl.when(ep < ep_size - 1)
    def _():
        halo_copy().wait_send()

    for offset in range(1, tp_size):
        pool_copy(offset).wait_send()
    for direction in range(2):

        @pl.when((has_left, has_right)[direction])
        def _(direction=direction):
            mix_copy(z, direction).wait_send()


    def drain(source, carry):
        @pl.when(~is_end(source) | (source == z))
        def _():
            for offset in range(1, ep_size):
                plane_copy(source, offset).wait_send()
                for index in range(PIECES):
                    back_copy(source, offset, index).wait_send()

        share_copy(source).wait_send()
        pair_copy(source).wait_send()

        @pl.when(is_end(source) & (~at_end | (source == z)))
        def _():
            for offset in range(ep_size):
                block_copy(source, offset).wait_send()

        @pl.when(is_end(source) & (source != z))
        def _():
            @pl.when(~at_end)
            def _():
                for index in range(PIECES - 1):
                    for half in range(2):
                        total_copy(source, index, half).wait_send()

            for half in range(2):
                total_copy(source, PIECES - 1, half).wait_send()

        for direction in range(2):
            toward = (source < z, source > z)[direction]
            has_next = (has_left, has_right)[direction]
            forwarded = (source > z, source < z)[direction]

            @pl.when(~is_end(source) & toward)
            def _(direction=direction):
                for index in range(PIECES):
                    sum_copy(source, source, index, direction).wait_send()

            @pl.when(~is_end(source) & forwarded & has_next)
            def _(direction=direction):
                line_copy(x_ref, source, direction).wait_send()

            @pl.when(forwarded & has_next)
            def _(direction=direction):
                mix_copy(source, direction).wait_send()

        return carry

    lax.fori_loop(0, planes, drain, 0)
    for slot in range(2):
        for index in range(PIECES):
            part_copy(0, slot, index).wait_send()


def fused_layers(extended, pool_input, pool_gain, mix_weight, weights, ep_size, planes, slots):
    gate_weight, up_weight, down_weight = weights
    rows, wide = extended.shape
    sequence, channels = pool_input.shape
    depth, outputs = mix_weight.shape
    tp_size = 2 * planes
    share_rows = sequence // tp_size
    edge = 16
    local_experts, width, ff = gate_weight.shape
    block = ep_size * slots
    piece = width // PIECES
    half = jnp.bfloat16
    dma = pltpu.SemaphoreType.DMA
    return pl.pallas_call(
        functools.partial(expert_kernel, ep_size, planes),
        out_shape=(
            jax.ShapeDtypeStruct((share_rows, outputs), half),
            jax.ShapeDtypeStruct((rows, width), half),
        ),
        in_specs=[pl.BlockSpec(memory_space=pltpu.VMEM)] * 3
        + [pl.BlockSpec(memory_space=pl.ANY)] * 4,
        out_specs=(pl.BlockSpec(memory_space=pltpu.VMEM),) * 2,
        scratch_shapes=[
            pltpu.VMEM((planes, rows, wide), half),
            pltpu.VMEM((planes, ep_size - 1, slots, wide), half),
            pltpu.VMEM((planes, 2, block, wide), half),
            pltpu.VMEM((local_experts, width, 2 * ff), half),
            pltpu.VMEM((width, local_experts * ff), half),
            pltpu.VMEM((2 * block, local_experts * ff), half),
            pltpu.VMEM((2, PIECES, block, piece), half),
            pltpu.VMEM((planes, PIECES, block, piece), half),
            pltpu.VMEM((2, PIECES, block, piece), half),
            pltpu.VMEM((planes, PIECES, block, piece), half),
            pltpu.VMEM((planes + 1, PIECES, rows, piece), half),
            dma((3 * local_experts,)),
            dma((planes, 2)),
            dma((planes,)),
            dma((planes, ep_size - 1)),
            dma((planes, ep_size - 1)),
            dma((planes,)),
            dma((planes,)),
            dma((2, PIECES)),
            dma((2, PIECES)),
            dma((planes, ep_size - 1, PIECES)),
            dma((planes, ep_size - 1, PIECES)),
            dma((planes, PIECES)),
            dma((planes, PIECES)),
            dma((planes, PIECES)),
            dma((planes, PIECES)),
            pltpu.VMEM((edge, channels), half),
            pltpu.VMEM((sequence, channels), half),
            pltpu.VMEM((share_rows, tp_size * channels), half),
            pltpu.VMEM((tp_size, depth, outputs), half),
            dma((2,)),
            dma,
            dma((tp_size - 1,)),
            dma((tp_size - 1,)),
            dma((planes, ep_size)),
            dma((planes, ep_size)),
            dma((planes, 2 * PIECES)),
            dma((planes, 2 * PIECES)),
            dma((planes, 2)),
            dma((planes,)),
            dma((planes,)),
            dma((planes,)),
        ],
        compiler_params=pltpu.CompilerParams(
            collective_id=0, has_side_effects=True, vmem_limit_bytes=VMEM_LIMIT
        ),
    )(extended, pool_input, pool_gain[None, :], mix_weight, gate_weight, up_weight, down_weight)


def routing_lanes(expert_ids, route_weight, ep_size):
    local_experts = EXPERTS // ep_size
    owners = expert_ids // local_experts
    ep_index = lax.iota(jnp.int32, ep_size)
    member = jnp.any(owners[:, :, None] == ep_index[None, None, :], axis=1)
    counts = member.astype(jnp.int32)
    rank = jnp.cumsum(counts, axis=0) - counts
    slot = jnp.where(member, rank, -1).astype(jnp.float32)
    within = expert_ids % local_experts
    named = within[:, :, None] == lax.iota(jnp.int32, local_experts)[None, None, :]
    weights = jnp.sum(jnp.where(named, route_weight[:, :, None], 0.0), axis=1)
    high = lax.reduce_precision(weights, 8, 7)
    low = weights - high
    spare = LANES - 2 * local_experts - ep_size
    lanes = jnp.concatenate([high, low, slot], axis=1)
    return jnp.pad(lanes, ((0, 0), (0, spare))).astype(jnp.bfloat16)


def fast_body(
    pool_input,
    pool_gain,
    mix_weight,
    moe_input,
    moe_gain,
    expert_ids,
    route_weight,
    gate_weight,
    up_weight,
    down_weight,
):
    ep_size = lax.axis_size("ep")
    planes = lax.axis_size("tp") // 2
    local_experts = gate_weight.shape[0]
    slots = local_experts * CAP // TOP
    inputs = moe_input.astype(jnp.float32)
    scale_rows = lax.rsqrt(jnp.mean(inputs * inputs, axis=-1, keepdims=True) + eps_norm)
    normed = (inputs * scale_rows * moe_gain).astype(jnp.bfloat16)
    extended = jnp.concatenate([normed, routing_lanes(expert_ids, route_weight, ep_size)], axis=1)
    return fused_layers(
        extended,
        pool_input,
        pool_gain,
        mix_weight,
        (gate_weight, up_weight, down_weight),
        ep_size,
        planes,
        slots,
    )


def fits(mesh, shapes):
    pool_input, mix_weight, moe_input, gate_weight = shapes
    ep_size = mesh.shape["ep"]
    tp_size = mesh.shape["tp"]
    experts, width, ff = gate_weight
    local_experts = experts // ep_size
    rows = moe_input[0] // (ep_size * tp_size)
    ff = ff // tp_size
    if local_experts % GROUP_EXP or tp_size != 8 or ep_size != 4 or ff % LANES or width % (PIECES * LANES):
        return False
    if 2 * local_experts + ep_size > LANES or rows > 256:
        return False
    slots = local_experts * CAP // TOP
    if slots % 16 or rows % 16:
        return False
    sequence = pool_input[0] // ep_size
    channels = pool_input[1] // tp_size
    share_rows = sequence // tp_size
    if channels % LANES or mix_weight[0] != pool_input[1] or share_rows % 16 or mix_weight[1] % LANES:
        return False
    mixer = mix_weight[0] * mix_weight[1] + share_rows * (mix_weight[0] + mix_weight[1])
    mixer += 2 * sequence * channels
    needed = kernel_bytes(ep_size, tp_size // 2, rows, slots, width, ff, local_experts, mixer)
    return needed < VMEM_LIMIT


def solution(mesh):
    def program(*arguments):
        shapes = tuple(arguments[index].shape for index in (0, 2, 3, 7))
        body = fast_body if fits(mesh, shapes) else general_body
        return jax.shard_map(
            body,
            mesh=mesh,
            in_specs=(
                P("ep", "tp"),
                P("tp"),
                P("tp", None),
                P(("ep", "tp"), None),
                P(),
                P(("ep", "tp"), None),
                P(("ep", "tp"), None),
                P("ep", None, "tp"),
                P("ep", None, "tp"),
                P("ep", None, "tp"),
            ),
            out_specs=(P(("ep", "tp"), None), P(("ep", "tp"), None)),
            check_vma=False,
        )(*arguments)

    return program
```

```python
import functools

import jax
import jax.numpy as jnp
from jax import lax
from jax.experimental import pallas as pl
from jax.experimental.pallas import tpu as pltpu
from jax.sharding import PartitionSpec as P

GROUP_CH = 256
EXPERTS = 16
GROUP_EXP = 4
TOP = 2
CAP = 48
CHUNKS = 2


eps_norm = 1e-06


def from_behind(shard, axis, by):
    peers = lax.axis_size(axis)
    pairs = [(i, i + by) for i in range(peers) if 0 <= i + by < peers]
    return lax.ppermute(shard, axis, pairs)


def window_sums(extended, row_count):
    level_sum = extended
    stride = 1
    outputs = []
    for doubling in range(4):
        level_sum = level_sum[stride:] + level_sum[:-stride]
        stride = stride * 2
        outputs.append(level_sum[level_sum.shape[0] - row_count :])
    return outputs


def pool_mixer(pool_input, pool_gain):
    row_count, channels = pool_input.shape
    carried = from_behind(pool_input[row_count - 15 :], "ep", 1)
    extended = jnp.concatenate([carried, pool_input], axis=0).astype(jnp.float32)
    window_list = window_sums(extended, row_count)
    channel_ids = lax.axis_index("tp") * channels + lax.iota(jnp.int32, channels)
    group_ids = channel_ids // GROUP_CH
    position = lax.axis_index("ep") * row_count + lax.iota(jnp.int32, row_count)
    summed = jnp.zeros((row_count, channels), jnp.float32)
    widths = jnp.zeros((channels,), jnp.int32)
    for index_group in range(4):
        inside = group_ids == index_group
        summed = jnp.where(inside[None, :], window_list[index_group], summed)
        widths = jnp.where(inside, 2 ** (index_group + 1), widths)
    counted = jnp.minimum(position[:, None] + 1, widths[None, :]).astype(jnp.float32)
    values = extended[15:]
    return ((summed / counted - values) * pool_gain).astype(jnp.bfloat16)


def dispatch_plan(expert_ids, route_weight, ep_size):
    local_experts = EXPERTS // ep_size
    share = TOP if local_experts % GROUP_EXP == 0 else 1
    capacity = local_experts * CAP // share
    owners = expert_ids // local_experts
    ep_index = lax.iota(jnp.int32, ep_size)
    member = jnp.any(owners[:, :, None] == ep_index[None, None, :], axis=1)
    counts = member.astype(jnp.int32)
    rank = jnp.cumsum(counts, axis=0) - counts
    slot = jnp.where(member, rank, -1).T
    placing = slot[:, None, :] == lax.iota(jnp.int32, capacity)[None, :, None]
    dense_weight = jnp.sum(
        jnp.where(
            expert_ids[:, :, None] == lax.iota(jnp.int32, EXPERTS)[None, None, :],
            route_weight[:, :, None],
            0.0,
        ),
        axis=1,
    )
    dense_weight = dense_weight.reshape(-1, ep_size, local_experts)
    slot_weight = jnp.einsum(
        "ecn,nej->ecj",
        placing.astype(jnp.float32),
        dense_weight,
        precision=lax.Precision.HIGHEST,
    )
    return placing.astype(jnp.bfloat16).reshape(ep_size * capacity, -1), slot_weight, capacity


def general_body(
    pool_input,
    pool_gain,
    mix_weight,
    moe_input,
    moe_gain,
    expert_ids,
    route_weight,
    gate_weight,
    up_weight,
    down_weight,
):
    pooled = pool_mixer(pool_input, pool_gain)
    ep_size = lax.axis_size("ep")
    out_columns = mix_weight.shape[1] // ep_size
    mix_columns = lax.dynamic_slice_in_dim(
        mix_weight, lax.axis_index("ep") * out_columns, out_columns, axis=1
    )
    mix_columns = lax.all_gather(mix_columns, "tp", axis=0, tiled=True)
    inputs = moe_input.astype(jnp.float32)
    scale_rows = lax.rsqrt(jnp.mean(inputs * inputs, axis=-1, keepdims=True) + eps_norm)
    normed = (inputs * scale_rows * moe_gain).astype(jnp.bfloat16)
    placing, slot_weight, capacity = dispatch_plan(expert_ids, route_weight, ep_size)
    rows = capacity // CHUNKS
    arrived_list = []
    placing_list = []
    for chunk in range(CHUNKS):
        chunk_placing = placing.reshape(ep_size, capacity, -1)[:, chunk * rows : (chunk + 1) * rows]
        chunk_placing = chunk_placing.reshape(ep_size * rows, -1)
        outgoing = jnp.dot(chunk_placing, normed, preferred_element_type=jnp.float32)
        outgoing = outgoing.astype(jnp.bfloat16)
        placing_list.append(chunk_placing)
        arrived_list.append(
            lax.all_to_all(outgoing, "ep", split_axis=0, concat_axis=0, tiled=True)
        )
    arrived_list[0], mix_columns = lax.optimization_barrier((arrived_list[0], mix_columns))
    weights = lax.all_to_all(slot_weight, "ep", split_axis=0, concat_axis=0, tiled=True)
    weights = lax.all_gather(weights, "tp", axis=0, tiled=True)
    combined = jnp.zeros(normed.shape, jnp.float32)
    for chunk in range(CHUNKS):
        tokens = lax.all_gather(arrived_list[chunk], "tp", axis=0, tiled=True)
        scales = weights[:, chunk * rows : (chunk + 1) * rows].reshape(tokens.shape[0], -1)
        gate_part = jnp.einsum(
            "nd,edf->enf", tokens, gate_weight, preferred_element_type=jnp.float32
        )
        upward = jnp.einsum("nd,edf->enf", tokens, up_weight, preferred_element_type=jnp.float32)
        hidden = (jax.nn.silu(gate_part) * upward * scales.T[:, :, None]).astype(jnp.bfloat16)
        partial = jnp.einsum("enf,edf->nd", hidden, down_weight, preferred_element_type=jnp.float32)
        reduced = lax.psum_scatter(
            partial.astype(jnp.bfloat16), "tp", scatter_dimension=0, tiled=True
        )
        returned = lax.all_to_all(reduced, "ep", split_axis=0, concat_axis=0, tiled=True)
        combined = combined + lax.dot_general(
            placing_list[chunk],
            returned,
            (((0,), (0,)), ((), ())),
            preferred_element_type=jnp.float32,
        )
    moe_out = combined.astype(jnp.bfloat16)
    regrouped = lax.all_to_all(pooled, "tp", split_axis=0, concat_axis=1, tiled=True)
    half = regrouped.shape[1] // 2
    mixed_sum = 0.0
    for part in range(2):
        section = slice(part * half, (part + 1) * half)
        pooled_rows = lax.all_gather(regrouped[:, section], "ep", axis=0, tiled=True)
        mixed_sum = mixed_sum + jnp.dot(
            pooled_rows, mix_columns[section], preferred_element_type=jnp.float32
        )
    mixed_out = lax.all_to_all(
        mixed_sum.astype(jnp.bfloat16), "ep", split_axis=0, concat_axis=1, tiled=True
    )
    return (mixed_out, moe_out)


LANES = 128
PIECES = 4
LAG = 2
VMEM_LIMIT = 67043328
MESH = pl.DeviceIdType.MESH


def kernel_bytes(ep_size, planes, rows, slots, width, hidden, local_experts, mixer_elements):
    wide = width + LANES
    block = ep_size * slots
    elements = planes * rows * wide
    elements += planes * (ep_size - 1) * slots * wide
    elements += planes * 2 * block * wide
    elements += 3 * local_experts * width * hidden
    elements += (planes * 2 + 4) * block * width
    elements += (planes + 1) * rows * width
    elements += 2 * block * local_experts * hidden
    elements += rows * (wide + width)
    elements += mixer_elements
    return 2 * elements


def expert_kernel(
    ep_size,
    planes,
    input_ref,
    scale_ref,
    routes_ref,
    pool_ref,
    gain_ref,
    mix_ref,
    gate_ref,
    up_ref,
    down_ref,
    mixed_ref,
    out_ref,
    column,
    packed,
    tokens,
    gate_up,
    down,
    hidden,
    outgoing,
    partial,
    arriving,
    returned,
    running,
    weight_sems,
    line_send,
    line_recv,
    plane_send,
    plane_recv,
    share_send,
    share_recv,
    part_send,
    part_recv,
    back_send,
    back_recv,
    left_send,
    right_send,
    left_recv,
    right_recv,
    halo,
    pooled,
    regrouped,
    mix,
    halo_sems,
    mix_load,
    pool_send,
    pool_recv,
    block_send,
    block_recv,
    total_send,
    total_recv,
    mix_send,
    mix_recv,
    pair_send,
    pair_recv,
):
    ep = lax.axis_index("ep")
    tp = lax.axis_index("tp")
    z = tp // 2
    core = tp % 2
    rows, width = input_ref.shape
    wide = width + LANES
    local_experts, _, ff = gate_ref.shape
    slots = packed.shape[2]
    block = ep_size * slots
    piece = width // PIECES
    partner = (ep, tp + 1 - 2 * core)
    left = (ep, tp - 2)
    right = (ep, tp + 2)
    has_left = z > 0
    has_right = z < planes - 1
    at_end = (z * (planes - 1 - z)) == 0
    turn = 1 - 2 * (z // (planes // 2))

    inner = (z * (planes - 1 - z) + planes - 2) // (planes - 1)

    def source_of(step):
        both_ways = ((step + 1) // 2) * (2 * (step % 2) - 1)
        far_first = step + (step // 2) * (1 - 2 * (step % 2))
        offset = inner * both_ways + (1 - inner) * far_first
        return (z + turn * offset + planes) % planes

    def is_end(source):
        return (source * (planes - 1 - source)) == 0

    def outward(source):
        return 1 - 2 * (source // (planes // 2))

    def peer_of(offset):
        return ((ep + offset) % ep_size, tp)

    tp_size = 2 * planes
    barrier = pltpu.get_barrier_semaphore()
    for offset in range(1, ep_size):
        pl.semaphore_signal(barrier, inc=1, device_id=peer_of(offset), device_id_type=MESH)
    for offset in range(1, tp_size):
        pl.semaphore_signal(
            barrier, inc=1, device_id=(ep, (tp + offset) % tp_size), device_id_type=MESH
        )

    loads = []
    for expert in range(local_experts):
        lanes = pl.ds(expert * ff, ff)
        loads.append((gate_ref.at[expert], gate_up.at[expert, :, pl.ds(0, ff)]))
        loads.append((up_ref.at[expert], gate_up.at[expert, :, pl.ds(ff, ff)]))
        loads.append((down_ref.at[expert], down.at[:, lanes]))
    loads = [
        pltpu.make_async_copy(source, target, weight_sems.at[index])
        for index, (source, target) in enumerate(loads)
    ]
    for load in loads:
        load.start()
    mix_own = pltpu.make_async_copy(mix_ref, mix.at[tp], mix_load)
    mix_own.start()
    x_ref = column.at[z]

    def normalize():
        values = input_ref[...].astype(jnp.float32)
        mean = jnp.mean(values * values, axis=-1, keepdims=True)
        values = values * lax.rsqrt(mean + eps_norm) * scale_ref[...]
        column[z, :, :width] = values.astype(jnp.bfloat16)

    def route():
        routes = routes_ref[...].T
        lane = lax.broadcasted_iota(jnp.int32, (rows, LANES), 1)
        place = (lane - 2 * local_experts).astype(jnp.float32)
        inside = (place >= 0) & (place < ep_size)
        within = jnp.where(lane < local_experts, lane, lane - local_experts).astype(jnp.float32)
        named = jnp.zeros((rows, LANES), jnp.float32)
        weights = jnp.zeros((rows, LANES), jnp.float32)
        for index in range(TOP):
            expert = routes[:, index : index + 1]
            weight = routes[:, TOP + index : TOP + index + 1]
            first = place * local_experts
            here = (expert >= first) & (expert < first + local_experts) & inside
            named = jnp.where(here, 1.0, named)
            for group in range(ep_size):
                chosen = expert == within + group * local_experts
                weights = weights + jnp.where(chosen, weight, 0.0)
        earlier = lax.broadcasted_iota(jnp.int32, (rows, rows), 1)
        later = lax.broadcasted_iota(jnp.int32, (rows, rows), 0)
        before = jnp.where(earlier < later, 1.0, 0.0).astype(jnp.bfloat16)
        rank = jnp.dot(before, named.astype(jnp.bfloat16), preferred_element_type=jnp.float32)
        slot = jnp.where(named > 0.5, rank, -1.0)
        high = weights.astype(jnp.bfloat16).astype(jnp.float32)
        lanes = jnp.where(inside, slot, 0.0)
        lanes = jnp.where(lane < 2 * local_experts, weights - high, lanes)
        lanes = jnp.where(lane < local_experts, high, lanes)
        column[z, :, width:] = lanes.astype(jnp.bfloat16)

    normalize()
    route()
    pl.semaphore_wait(barrier, ep_size + tp_size - 2)

    def line_copy(source_ref, source, direction):
        return pltpu.make_async_remote_copy(
            src_ref=source_ref,
            dst_ref=column.at[source],
            send_sem=line_send.at[source, direction],
            recv_sem=line_recv.at[source],
            device_id=(left, right)[direction],
            device_id_type=MESH,
        )

    def plane_copy(source, offset):
        return pltpu.make_async_remote_copy(
            src_ref=packed.at[source, offset - 1],
            dst_ref=tokens.at[source, core, pl.ds(pl.multiple_of(ep * slots, slots), slots)],
            send_sem=plane_send.at[source, offset - 1],
            recv_sem=plane_recv.at[source, offset - 1],
            device_id=peer_of(offset),
            device_id_type=MESH,
        )

    def share_copy(source):
        return pltpu.make_async_remote_copy(
            src_ref=tokens.at[source, core],
            dst_ref=tokens.at[source, core],
            send_sem=share_send.at[source],
            recv_sem=share_recv.at[source],
            device_id=partner,
            device_id_type=MESH,
        )

    def part_copy(source, slot, index):
        return pltpu.make_async_remote_copy(
            src_ref=outgoing.at[slot, index],
            dst_ref=arriving.at[slot, index],
            send_sem=part_send.at[slot, index],
            recv_sem=part_recv.at[slot, index],
            device_id=partner,
            device_id_type=MESH,
        )

    def back_copy(source, offset, index):
        target = (ep + offset) % ep_size
        return pltpu.make_async_remote_copy(
            src_ref=partial.at[source, index, pl.ds(pl.multiple_of(target * slots, slots), slots)],
            dst_ref=returned.at[source, index, pl.ds(pl.multiple_of(ep * slots, slots), slots)],
            send_sem=back_send.at[source, offset - 1, index],
            recv_sem=back_recv.at[source, offset - 1, index],
            device_id=(target, tp),
            device_id_type=MESH,
        )

    def sum_copy(source, place, index, direction):
        return pltpu.make_async_remote_copy(
            src_ref=running.at[source, index],
            dst_ref=running.at[place, index],
            send_sem=(left_send, right_send)[direction].at[source, index],
            recv_sem=(right_recv, left_recv)[direction].at[source, index],
            device_id=(left, right)[direction],
            device_id_type=MESH,
        )

    def sum_place(source, direction):
        if direction == 1:
            return source
        ends = (source + 1) // jnp.maximum(z, 1)
        return source + (planes - source) * ends

    def block_copy(source, offset):
        start = pl.multiple_of(((ep - offset + ep_size) % ep_size) * slots, slots)
        return pltpu.make_async_remote_copy(
            src_ref=tokens.at[source, core, pl.ds(start, slots)],
            dst_ref=tokens.at[source, core, pl.ds(start, slots)],
            send_sem=block_send.at[source, offset],
            recv_sem=block_recv.at[source, offset],
            device_id=(ep, tp + 2 * outward(source)),
            device_id_type=MESH,
        )

    def half_rows(half):
        return pl.ds(half * (block // 2), block // 2)

    def total_copy(source, index, half):
        hops = (z - source) * outward(source)
        place = source + (planes - 1 - 2 * source) * ((planes - hops) // (planes - 1))
        return pltpu.make_async_remote_copy(
            src_ref=partial.at[source, index, half_rows(half)],
            dst_ref=returned.at[place, index, half_rows(half)],
            send_sem=total_send.at[source, 2 * index + half],
            recv_sem=total_recv.at[source, 2 * index + half],
            device_id=(ep, tp - 2 * outward(source)),
            device_id_type=MESH,
        )

    def receive_block(source, offset):
        block_copy(source, offset).wait_recv()

        @pl.when(~at_end)
        def _():
            block_copy(source, offset).start()

    sequence, channels = pool_ref.shape
    share_rows = sequence // tp_size
    edge = halo.shape[0]

    def halo_copy():
        return pltpu.make_async_remote_copy(
            src_ref=pool_ref.at[pl.ds(sequence - edge, edge)],
            dst_ref=halo,
            send_sem=halo_sems.at[0],
            recv_sem=halo_sems.at[1],
            device_id=peer_of(1),
            device_id_type=MESH,
        )

    def pool_copy(offset):
        target = (tp + offset) % tp_size
        lanes = pl.ds(pl.multiple_of(tp * channels, channels), channels)
        return pltpu.make_async_remote_copy(
            src_ref=pooled.at[pl.ds(pl.multiple_of(target * share_rows, share_rows), share_rows)],
            dst_ref=regrouped.at[:, lanes],
            send_sem=pool_send.at[offset - 1],
            recv_sem=pool_recv.at[offset - 1],
            device_id=(ep, target),
            device_id_type=MESH,
        )

    def mix_copy(plane, direction):
        return pltpu.make_async_remote_copy(
            src_ref=mix.at[2 * plane + core],
            dst_ref=mix.at[2 * plane + core],
            send_sem=mix_send.at[plane, direction],
            recv_sem=mix_recv.at[plane],
            device_id=(left, right)[direction],
            device_id_type=MESH,
        )

    def pair_copy(plane):
        return pltpu.make_async_remote_copy(
            src_ref=mix.at[2 * plane + core],
            dst_ref=mix.at[2 * plane + core],
            send_sem=pair_send.at[plane],
            recv_sem=pair_recv.at[plane],
            device_id=partner,
            device_id_type=MESH,
        )

    def send_mix():
        @pl.when(has_left)
        def _():
            mix_copy(z, 0).start()

        @pl.when(has_right)
        def _():
            mix_copy(z, 1).start()

        pair_copy(z).start()

    def receive_mix(plane):
        mix_copy(plane, 0).wait_recv()

        @pl.when((plane > z) & has_left)
        def _():
            mix_copy(plane, 0).start()

        @pl.when((plane < z) & has_right)
        def _():
            mix_copy(plane, 1).start()

        pair_copy(plane).start()

    def pool():
        @pl.when(ep > 0)
        def _():
            halo_copy().wait_recv()

        before = jnp.where(ep > 0, halo[...].astype(jnp.float32), 0.0)
        values = pool_ref[...].astype(jnp.float32)
        level = jnp.concatenate([before, values], axis=0)
        channel = tp * channels + lax.broadcasted_iota(jnp.int32, (1, channels), 1)
        position = ep * sequence + lax.broadcasted_iota(jnp.int32, (sequence, 1), 0)
        summed = jnp.zeros((sequence, channels), jnp.float32)
        widths = jnp.zeros((1, channels), jnp.int32)
        for index in range(4):
            level = level + pltpu.roll(level, 2**index, 0)
            inside = (channel >= index * GROUP_CH) & (channel < (index + 1) * GROUP_CH)
            summed = jnp.where(inside, level[edge:], summed)
            widths = jnp.where(inside, 2 ** (index + 1), widths)
        counted = jnp.minimum(position + 1, widths).astype(jnp.float32)
        result = (summed / counted - values) * gain_ref[...]
        pooled[...] = result.astype(jnp.bfloat16)
        own_rows = pl.ds(pl.multiple_of(tp * share_rows, share_rows), share_rows)
        lanes = pl.ds(pl.multiple_of(tp * channels, channels), channels)
        regrouped[:, lanes] = pooled[own_rows]

    def send_pooled():
        for offset in range(1, tp_size):
            pool_copy(offset).start()

    def mixer():
        for offset in range(1, tp_size):
            pool_copy(offset).wait_recv()
        for plane in range(planes):
            pair_copy(plane).wait_recv()
        total = jnp.zeros((share_rows, mix.shape[2]), jnp.float32)
        for index in range(tp_size):
            part = regrouped[:, index * channels : (index + 1) * channels]
            total = total + jnp.dot(part, mix[index], preferred_element_type=jnp.float32)
        mixed_ref[...] = total.astype(jnp.bfloat16)

    def dispatch(source_ref, source):
        routing = source_ref[:, width:].astype(jnp.float32).T
        for offset in range(ep_size):
            group = (ep + offset) % ep_size
            slot_row = jnp.zeros((1, rows), jnp.float32)
            for index in range(ep_size):
                row = 2 * local_experts + index
                chosen = jnp.where(index == group, 1.0, 0.0)
                slot_row = slot_row + routing[row : row + 1] * chosen
            places = lax.broadcasted_iota(jnp.int32, (slots, rows), 0).astype(jnp.float32)
            placing = jnp.where(places == slot_row, 1.0, 0.0).astype(jnp.bfloat16)
            compact = jnp.dot(placing, source_ref[...], preferred_element_type=jnp.float32)
            compact = compact.astype(jnp.bfloat16)
            if offset == 0:
                tokens[source, core, pl.ds(pl.multiple_of(ep * slots, slots), slots)] = compact
            else:
                packed[source, offset - 1] = compact
                plane_copy(source, offset).start()

    def gather(source):
        for offset in range(1, ep_size):
            plane_copy(source, offset).wait_recv()
        share_copy(source).start()

    def keep_own(source, index):
        own_rows = pl.ds(pl.multiple_of(ep * slots, slots), slots)
        returned[source, index, own_rows] = partial[source, index, own_rows]

    def experts(source, slot):
        share_copy(source).wait_recv()

        def one(expert, carry):
            values = tokens[source].reshape(2 * block, wide)
            both = jnp.dot(
                values[:, :width], gate_up[expert], preferred_element_type=jnp.float32
            )
            lane = lax.broadcasted_iota(jnp.int32, (2 * block, LANES), 1)
            mine = (lane == expert) | (lane == local_experts + expert)
            scale = jnp.where(mine, values[:, width:].astype(jnp.float32), 0.0)
            scale = jnp.sum(scale, axis=1, keepdims=True)
            gated = both[:, :ff]
            gated = gated / (1.0 + jnp.exp(-gated))
            result = (gated * both[:, ff:] * scale).astype(jnp.bfloat16)
            hidden[:, pl.ds(pl.multiple_of(expert * ff, ff), ff)] = result
            return carry

        lax.fori_loop(0, local_experts, one, 0)

        def project(which, index):
            part = hidden[pl.ds(pl.multiple_of(which * block, block), block)]
            return lax.dot_general(
                part,
                down[index * piece : (index + 1) * piece],
                (((1,), (1,)), ((), ())),
                preferred_element_type=jnp.float32,
            )

        for index in range(PIECES):
            outgoing[slot, index] = project(1 - core, index).astype(jnp.bfloat16)
            part_copy(source, slot, index).start()
        for index in range(PIECES):
            own = project(core, index)
            part_copy(source, slot, index).wait_recv()
            total = own + arriving[slot, index].astype(jnp.float32)
            partial[source, index] = total.astype(jnp.bfloat16)

            @pl.when(~is_end(source))
            def _():
                keep_own(source, index)

            @pl.when(~is_end(source))
            def _():
                for offset in range(1, ep_size):
                    back_copy(source, offset, index).start()

            @pl.when(is_end(source) & at_end & (source != z))
            def _():
                for half in range(2):
                    total_copy(source, index, half).start()

    def placing_back(source_ref):
        routing = source_ref[:, width:].astype(jnp.float32)
        pieces = []
        for group in range(ep_size):
            lane = 2 * local_experts + group
            places = lax.broadcasted_iota(jnp.int32, (rows, slots), 1).astype(jnp.float32)
            matched = places == routing[:, lane : lane + 1]
            pieces.append(jnp.where(matched, 1.0, 0.0))
        return jnp.concatenate(pieces, axis=1).astype(jnp.bfloat16)

    def combine(placing, source, index):
        for offset in range(1, ep_size):
            back_copy(source, offset, index).wait_recv()
        return jnp.dot(placing, returned[source, index], preferred_element_type=jnp.float32)

    def reduce_piece(source, placing, index):
        mine = combine(placing, source, index)
        for direction in range(2):
            toward = (source < z, source > z)[direction]
            has_before = (has_right, has_left)[direction]

            @pl.when(toward & has_before)
            def _(direction=direction):
                sum_copy(source, source, index, direction).wait_recv()
                total = mine + running[source, index].astype(jnp.float32)
                running[source, index] = total.astype(jnp.bfloat16)
                place = sum_place(source, direction)
                sum_copy(source, place, index, direction).start()

            @pl.when(toward & ~has_before)
            def _(direction=direction):
                running[source, index] = mine.astype(jnp.bfloat16)
                place = sum_place(source, direction)
                sum_copy(source, place, index, direction).start()

    def reduce_line(source):
        placing = placing_back(column.at[source])
        for index in range(PIECES):
            reduce_piece(source, placing, index)

    def add_total(source, place, index, half):
        total_copy(source, index, half).wait_recv()
        which = half_rows(half)
        total = partial[source, index, which].astype(jnp.float32)
        total = total + returned[place, index, which].astype(jnp.float32)
        partial[source, index, which] = total.astype(jnp.bfloat16)

    def pass_total(source, index, half):
        add_total(source, source, index, half)
        total_copy(source, index, half).start()

    def receive(source):
        line_copy(x_ref, source, 0).wait_recv()

        @pl.when((source > z) & has_left)
        def _():
            line_copy(column.at[source], source, 0).start()

        @pl.when((source < z) & has_right)
        def _():
            line_copy(column.at[source], source, 1).start()

    @pl.when(~at_end)
    def _():
        line_copy(x_ref, z, 0).start()
        line_copy(x_ref, z, 1).start()

    @pl.when(ep < ep_size - 1)
    def _():
        halo_copy().start()

    dispatch(x_ref, z)

    @pl.when(at_end)
    def _():
        block_copy(z, 0).start()

    pool()

    @pl.when(at_end)
    def _():
        for offset in range(1, ep_size):
            plane_copy(z, offset).wait_recv()
            block_copy(z, offset).start()
        share_copy(z).start()

    mix_own.wait()
    for load in loads:
        load.wait()

    def step_body(step, carry):
        current = source_of(step)
        slot = step % 2

        @pl.when(step == 0)
        def _():
            receive(source_of(1))
            dispatch(column.at[source_of(1)], source_of(1))

        @pl.when(at_end & (step == 1))
        def _():
            send_mix()
            send_pooled()

        @pl.when(at_end & (step == 2))
        def _():
            reduce_line(source_of(1))

        @pl.when(~at_end & (step == 0))
        def _():
            receive_block(source_of(2), 0)
            receive_block(source_of(2), 1)

        @pl.when(~at_end & (step == 1))
        def _():
            receive_block(source_of(2), 2)
            receive_block(source_of(2), 3)
            receive_block(source_of(3), 0)

        @pl.when(~is_end(current))
        def _():
            gather(current)

        @pl.when(~at_end & (step == 1))
        def _():
            receive_block(source_of(3), 1)

        @pl.when(~at_end & (step == 2))
        def _():
            receive_block(source_of(3), 2)

        @pl.when(~at_end & (step == 3))
        def _():
            receive_block(source_of(3), 3)
            send_mix()
            send_pooled()
            receive_mix(source_of(2))

        @pl.when(at_end & (step == 2))
        def _():
            for offset in range(ep_size):
                receive_block(current, offset)

        @pl.when(is_end(current) & (current != z))
        def _():
            share_copy(current).start()

        @pl.when(step > 1)
        def _():
            for index in range(PIECES):
                part_copy(current, slot, index).wait_send()

        experts(current, slot)

        @pl.when(at_end & (step == 1))
        def _():
            receive(source_of(3))
            dispatch(column.at[source_of(3)], source_of(3))

        return carry

    lax.fori_loop(0, planes, step_body, 0)

    @pl.when(at_end)
    def _():
        reduce_line(source_of(3))
        for step in range(1, planes):
            receive_mix(source_of(step))
        for index in range(PIECES):
            for half in range(2):
                add_total(z, planes - 1 - z, index, half)
            keep_own(z, index)
            for offset in range(1, ep_size):
                back_copy(z, offset, index).start()

    @pl.when(~at_end)
    def _():
        receive_mix(source_of(1))
        receive_mix(source_of(3))
        for count in range(2 * PIECES + LAG):
            if count < 2 * PIECES:
                pass_total(source_of(3), count // 2, count % 2)
            if count >= LAG:
                pass_total(source_of(2), (count - LAG) // 2, (count - LAG) % 2)
        reduce_line(source_of(1))

    mixer()

    placing = placing_back(x_ref)
    for index in range(PIECES):
        mine = combine(placing, z, index)
        lanes = pl.ds(index * piece, piece)

        @pl.when(~at_end)
        def _():
            sum_copy(z, z, index, 0).wait_recv()
            sum_copy(z, z, index, 1).wait_recv()
            others = running[z, index].astype(jnp.float32)
            others = others + running[planes, index].astype(jnp.float32)
            out_ref[:, lanes] = (mine + others).astype(jnp.bfloat16)

        @pl.when(at_end)
        def _():
            out_ref[:, lanes] = mine.astype(jnp.bfloat16)

    @pl.when(~at_end)
    def _():
        line_copy(x_ref, z, 0).wait_send()
        line_copy(x_ref, z, 1).wait_send()

    @pl.when(ep < ep_size - 1)
    def _():
        halo_copy().wait_send()

    for offset in range(1, tp_size):
        pool_copy(offset).wait_send()
    for direction in range(2):

        @pl.when((has_left, has_right)[direction])
        def _(direction=direction):
            mix_copy(z, direction).wait_send()


    def drain(source, carry):
        @pl.when(~is_end(source) | (source == z))
        def _():
            for offset in range(1, ep_size):
                plane_copy(source, offset).wait_send()
                for index in range(PIECES):
                    back_copy(source, offset, index).wait_send()

        share_copy(source).wait_send()
        pair_copy(source).wait_send()

        @pl.when(is_end(source) & (~at_end | (source == z)))
        def _():
            for offset in range(ep_size):
                block_copy(source, offset).wait_send()

        @pl.when(is_end(source) & (source != z))
        def _():
            for index in range(PIECES):
                for half in range(2):
                    total_copy(source, index, half).wait_send()

        for direction in range(2):
            toward = (source < z, source > z)[direction]
            has_next = (has_left, has_right)[direction]
            forwarded = (source > z, source < z)[direction]

            @pl.when(~is_end(source) & toward)
            def _(direction=direction):
                for index in range(PIECES):
                    sum_copy(source, source, index, direction).wait_send()

            @pl.when(~is_end(source) & forwarded & has_next)
            def _(direction=direction):
                line_copy(x_ref, source, direction).wait_send()

            @pl.when(forwarded & has_next)
            def _(direction=direction):
                mix_copy(source, direction).wait_send()

        return carry

    lax.fori_loop(0, planes, drain, 0)
    for slot in range(2):
        for index in range(PIECES):
            part_copy(0, slot, index).wait_send()


def fused_layers(tokens, pool_input, pool_gain, mix_weight, weights, ep_size, planes, slots):
    gate_weight, up_weight, down_weight = weights
    moe_input, moe_gain, routes = tokens
    rows, width = moe_input.shape
    wide = width + LANES
    sequence, channels = pool_input.shape
    depth, outputs = mix_weight.shape
    tp_size = 2 * planes
    share_rows = sequence // tp_size
    edge = 16
    local_experts, _, ff = gate_weight.shape
    block = ep_size * slots
    piece = width // PIECES
    half = jnp.bfloat16
    dma = pltpu.SemaphoreType.DMA
    return pl.pallas_call(
        functools.partial(expert_kernel, ep_size, planes),
        out_shape=(
            jax.ShapeDtypeStruct((share_rows, outputs), half),
            jax.ShapeDtypeStruct((rows, width), half),
        ),
        in_specs=[pl.BlockSpec(memory_space=pltpu.VMEM)] * 5
        + [pl.BlockSpec(memory_space=pl.ANY)] * 4,
        out_specs=(pl.BlockSpec(memory_space=pltpu.VMEM),) * 2,
        scratch_shapes=[
            pltpu.VMEM((planes, rows, wide), half),
            pltpu.VMEM((planes, ep_size - 1, slots, wide), half),
            pltpu.VMEM((planes, 2, block, wide), half),
            pltpu.VMEM((local_experts, width, 2 * ff), half),
            pltpu.VMEM((width, local_experts * ff), half),
            pltpu.VMEM((2 * block, local_experts * ff), half),
            pltpu.VMEM((2, PIECES, block, piece), half),
            pltpu.VMEM((planes, PIECES, block, piece), half),
            pltpu.VMEM((2, PIECES, block, piece), half),
            pltpu.VMEM((planes, PIECES, block, piece), half),
            pltpu.VMEM((planes + 1, PIECES, rows, piece), half),
            dma((3 * local_experts,)),
            dma((planes, 2)),
            dma((planes,)),
            dma((planes, ep_size - 1)),
            dma((planes, ep_size - 1)),
            dma((planes,)),
            dma((planes,)),
            dma((2, PIECES)),
            dma((2, PIECES)),
            dma((planes, ep_size - 1, PIECES)),
            dma((planes, ep_size - 1, PIECES)),
            dma((planes, PIECES)),
            dma((planes, PIECES)),
            dma((planes, PIECES)),
            dma((planes, PIECES)),
            pltpu.VMEM((edge, channels), half),
            pltpu.VMEM((sequence, channels), half),
            pltpu.VMEM((share_rows, tp_size * channels), half),
            pltpu.VMEM((tp_size, depth, outputs), half),
            dma((2,)),
            dma,
            dma((tp_size - 1,)),
            dma((tp_size - 1,)),
            dma((planes, ep_size)),
            dma((planes, ep_size)),
            dma((planes, 2 * PIECES)),
            dma((planes, 2 * PIECES)),
            dma((planes, 2)),
            dma((planes,)),
            dma((planes,)),
            dma((planes,)),
        ],
        compiler_params=pltpu.CompilerParams(
            collective_id=0, has_side_effects=True, vmem_limit_bytes=VMEM_LIMIT
        ),
    )(
        moe_input,
        moe_gain[None, :],
        routes,
        pool_input,
        pool_gain[None, :],
        mix_weight,
        gate_weight,
        up_weight,
        down_weight,
    )


def fast_body(
    pool_input,
    pool_gain,
    mix_weight,
    moe_input,
    moe_gain,
    expert_ids,
    route_weight,
    gate_weight,
    up_weight,
    down_weight,
):
    ep_size = lax.axis_size("ep")
    planes = lax.axis_size("tp") // 2
    local_experts = gate_weight.shape[0]
    slots = local_experts * CAP // TOP
    routes = jnp.concatenate([expert_ids.T.astype(jnp.float32), route_weight.T], axis=0)
    routes = jnp.pad(routes, ((0, 8 - 2 * TOP), (0, 0)))
    return fused_layers(
        (moe_input, moe_gain, routes),
        pool_input,
        pool_gain,
        mix_weight,
        (gate_weight, up_weight, down_weight),
        ep_size,
        planes,
        slots,
    )


def fits(mesh, shapes):
    pool_input, mix_weight, moe_input, gate_weight = shapes
    ep_size = mesh.shape["ep"]
    tp_size = mesh.shape["tp"]
    experts, width, ff = gate_weight
    local_experts = experts // ep_size
    rows = moe_input[0] // (ep_size * tp_size)
    ff = ff // tp_size
    if local_experts % GROUP_EXP or tp_size != 8 or ep_size != 4 or ff % LANES or width % (PIECES * LANES):
        return False
    if 2 * local_experts + ep_size > LANES or rows > 256:
        return False
    slots = local_experts * CAP // TOP
    if slots % 16 or rows % 16:
        return False
    sequence = pool_input[0] // ep_size
    channels = pool_input[1] // tp_size
    share_rows = sequence // tp_size
    if channels % LANES or mix_weight[0] != pool_input[1] or share_rows % 16 or mix_weight[1] % LANES:
        return False
    mixer = mix_weight[0] * mix_weight[1] + share_rows * (mix_weight[0] + mix_weight[1])
    mixer += 2 * sequence * channels
    needed = kernel_bytes(ep_size, tp_size // 2, rows, slots, width, ff, local_experts, mixer)
    return needed < VMEM_LIMIT


def solution(mesh):
    def program(*arguments):
        shapes = tuple(arguments[index].shape for index in (0, 2, 3, 7))
        body = fast_body if fits(mesh, shapes) else general_body
        return jax.shard_map(
            body,
            mesh=mesh,
            in_specs=(
                P("ep", "tp"),
                P("tp"),
                P("tp", None),
                P(("ep", "tp"), None),
                P(),
                P(("ep", "tp"), None),
                P(("ep", "tp"), None),
                P("ep", None, "tp"),
                P("ep", None, "tp"),
                P("ep", None, "tp"),
            ),
            out_specs=(P(("ep", "tp"), None), P(("ep", "tp"), None)),
            check_vma=False,
        )(*arguments)

    return program
```
